32 devices in a mesh: sp: 8 (over z, y), tp: 4 (over x, core).
Axes of the slice: x: 2, y: 2, z: 4, core: 2. Of those that a mesh axis runs over, the one named last changes fastest.
Arguments:
- latent: bfloat16 [1024, 4096], P(('sp', 'tp')), may hold values from -8 to 8
- context: bfloat16 [256, 4096], P('sp'), may hold values from -6 to 6
- condition: float32 [4096], P('sp'), may hold values from -6 to 6
- context_condition: float32 [4096], P('sp'), may hold values from -6 to 6
- shift_weight: bfloat16 [4096, 4096], P('sp', 'tp'), may hold values from -0.09375 to 0.09375
- scale_weight: bfloat16 [4096, 4096], P('sp', 'tp'), may hold values from -0.09375 to 0.09375
- gate_weight: bfloat16 [4096, 4096], P('sp', 'tp'), may hold values from -0.09375 to 0.09375
- norm_gain: float32 [4096], replicated, may hold values from 0.1 to 1.9
- decay_down: bfloat16 [4096, 128], replicated, may hold values from -0.09375 to 0.09375
- decay_up: bfloat16 [128, 4096], P(None, 'tp'), may hold values from -0.5 to 0.5
- rate_down: bfloat16 [4096, 128], replicated, may hold values from -0.09375 to 0.09375
- rate_up: bfloat16 [128, 4096], P(None, 'tp'), may hold values from -0.5 to 0.5
- head_bias: float32 [2, 4096], P(None, 'tp'), may hold values from -12 to 1
- query_weight: bfloat16 [4096, 4096], P(None, 'tp'), may hold values from -0.09375 to 0.09375
- key_weight: bfloat16 [4096, 4096], P(None, 'tp'), may hold values from -0.09375 to 0.09375
- value_weight: bfloat16 [4096, 4096], P(None, 'tp'), may hold values from -0.09375 to 0.09375
- branch_weight: bfloat16 [4096, 4096], P(None, 'tp'), may hold values from -0.09375 to 0.09375
- group_gain: float32 [4096], P('tp'), may hold values from 0.1 to 1.9
- out_weight: bfloat16 [4096, 4096], P('tp'), may hold values from -0.09375 to 0.09375
Outputs:
- updated: bfloat16 [1024, 4096], P(('sp', 'tp'))
The draws below stay inside these ranges and needn't reach their ends.
All inputs are finite; a program needn't handle non-finite values.
Results may differ from the reference program's by a relative error of at most 0.017.
Values may be sent and summed in bfloat16 or wider, within the bound.
No kernel may reach another device: no remote copies, remote signals or barrier semaphores. Data moves between devices by JAX's collectives and lax.ppermute only.
A program may use at most 192 MiB of HBM per device.

```python
import math
import jax
import jax.numpy as jnp
from jax import lax

D = 4096
HEAD_DIM = 64
RANK = 128
TOKENS = 1024
CONTEXT = 256
N_TP = 4


def draw_latent(key, part):
    base_key = jax.random.fold_in(key, 11)
    shared = jax.random.normal(jax.random.fold_in(base_key, 2), (TOKENS // 64, 1, D), jnp.float32)
    shared = jnp.broadcast_to(shared, (TOKENS // 64, 64, D)).reshape(TOKENS, D)
    noise = jax.random.normal(jax.random.fold_in(base_key, 1), (TOKENS, D), jnp.float32)
    value = noise + 0.8 * shared
    return jnp.clip(value, -8.0, 8.0).astype(jnp.bfloat16)


def draw_head_bias(key, part):
    base_key = jax.random.fold_in(key, 23)
    heads = D // HEAD_DIM
    share = 0.5
    decay_low_end = -12.0
    decay_high_end = -10.0
    rate_low_end = -9.0
    rate_high_end = -7.0
    slow_heads = jax.random.bernoulli(jax.random.fold_in(base_key, 1), share, (heads,))
    slow = jnp.repeat(slow_heads, HEAD_DIM)
    decay_fast = jax.random.uniform(jax.random.fold_in(base_key, 2), (D,), jnp.float32, minval=-4.5, maxval=-2.5)
    decay_slow = jax.random.uniform(jax.random.fold_in(base_key, 3), (D,), jnp.float32, minval=decay_low_end, maxval=decay_high_end)
    rate_fast = jax.random.uniform(jax.random.fold_in(base_key, 4), (D,), jnp.float32, minval=-1.0, maxval=1.0)
    rate_slow = jax.random.uniform(jax.random.fold_in(base_key, 5), (D,), jnp.float32, minval=rate_low_end, maxval=rate_high_end)
    decay_row = jnp.where(slow, decay_slow, decay_fast)
    rate_row = jnp.where(slow, rate_slow, rate_fast)
    return jnp.stack([decay_row, rate_row]).astype(jnp.float32)


def levels(stream_key, extent, pieces, low, largest):
    factor_of, own = 1.0, jax.random.fold_in(stream_key, 6)
    for axis_at, blocks in pieces:
        heights = jnp.exp(jax.random.uniform(jax.random.fold_in(own, axis_at), (blocks,), jnp.float32, low / len(pieces), largest / len(pieces)))
        factor_of = factor_of * jnp.repeat(heights, extent[axis_at] // blocks).reshape([-1 if axis == axis_at else 1 for axis in range(len(extent))])
    return factor_of


def centred(own_key, dims, scale, most, pieces=(), dtype=jnp.bfloat16):
    level = levels(own_key, dims, pieces, -0.22, 0.18) if pieces else 1.0
    values = jax.random.normal(own_key, dims, jnp.float32) * scale * level
    return jnp.minimum(jnp.maximum(values, -most), most).astype(dtype)


def setup_inputs(seed: int = 0) -> dict:
    arg_keys = jax.random.split(jax.random.key(seed), 20)
    return {
        "latent": draw_latent(jax.random.fold_in(arg_keys[19], 71), 0),
        "context": centred(arg_keys[1], (CONTEXT, D), 1.0, 6.0, ((0, 8),)),
        "condition": centred(arg_keys[2], (D,), 1.5, 6.0, ((0, 8),), jnp.float32),
        "context_condition": centred(arg_keys[3], (D,), 1.5, 6.0, ((0, 8),), jnp.float32),
        "shift_weight": centred(arg_keys[4], (D, D), D ** -0.5, 0.09375, ((0, 8), (1, 4))),
        "scale_weight": centred(arg_keys[5], (D, D), D ** -0.5, 0.09375, ((0, 8), (1, 4))),
        "gate_weight": centred(arg_keys[6], (D, D), D ** -0.5, 0.09375, ((0, 8), (1, 4))),
        "norm_gain": jnp.clip(1.0 + 0.18 * jax.random.normal(arg_keys[7], (D,), jnp.float32), 0.1, 1.9),
        "decay_down": centred(arg_keys[8], (D, RANK), D ** -0.5, 0.09375),
        "decay_up": centred(arg_keys[9], (RANK, D), RANK ** -0.5, 0.5, ((1, 4),)),
        "rate_down": centred(arg_keys[10], (D, RANK), D ** -0.5, 0.09375),
        "rate_up": centred(arg_keys[11], (RANK, D), RANK ** -0.5, 0.5, ((1, 4),)),
        "head_bias": draw_head_bias(jax.random.fold_in(arg_keys[19], 71), 0),
        "query_weight": centred(arg_keys[13], (D, D), D ** -0.5, 0.09375, ((1, 4),)),
        "key_weight": centred(arg_keys[14], (D, D), D ** -0.5, 0.09375, ((1, 4),)),
        "value_weight": centred(arg_keys[15], (D, D), D ** -0.5, 0.09375, ((1, 4),)),
        "branch_weight": centred(arg_keys[16], (D, D), D ** -0.5, 0.09375, ((1, 4),)),
        "group_gain": jnp.clip(1.0 + 0.18 * jax.random.normal(arg_keys[17], (D,), jnp.float32), 0.1, 1.9),
        "out_weight": centred(arg_keys[18], (D, D), D ** -0.5, 0.09375, ((0, 4),)),
    }


NORM_EPS = 1e-06
GROUP_EPS = 0.00064
DECAY_TOP = math.exp(-0.5)
highest = lax.Precision.HIGHEST

def modulated(rows, gain, scale, shift):
    values = rows.astype(jnp.float32)
    inverse = lax.rsqrt(lax.optimization_barrier(jnp.mean(values * values, axis=-1, keepdims=True)) + NORM_EPS)
    return (values * inverse * gain * (1.0 + scale) + shift).astype(jnp.bfloat16)

def features(normed, key_weight, value_weight, decay_down, decay_up, rate_down, rate_up):
    keys = jnp.dot(normed, key_weight, preferred_element_type=jnp.float32).astype(jnp.bfloat16)
    values = jnp.dot(normed, value_weight, preferred_element_type=jnp.float32).astype(jnp.bfloat16)
    decay_low = jnp.tanh(jnp.dot(normed, decay_down, preferred_element_type=jnp.float32)).astype(jnp.bfloat16)
    rate_low = jnp.dot(normed, rate_down, preferred_element_type=jnp.float32).astype(jnp.bfloat16)
    decay_pre = jnp.dot(decay_low, decay_up, preferred_element_type=jnp.float32).astype(jnp.bfloat16)
    rate_pre = jnp.dot(rate_low, rate_up, preferred_element_type=jnp.float32).astype(jnp.bfloat16)
    return (keys, values, decay_pre, rate_pre)

def chain_inputs(keys, values, decay_pre, rate_pre, head_bias):
    rows = keys.shape[0]
    log_decay = -DECAY_TOP * jax.nn.sigmoid(head_bias[0] + decay_pre.astype(jnp.float32))
    rate = jax.nn.sigmoid(head_bias[1] + rate_pre.astype(jnp.float32))
    key_heads = keys.astype(jnp.float32).reshape(rows, -1, HEAD_DIM)
    unit = key_heads * lax.rsqrt(lax.optimization_barrier(jnp.sum(key_heads * key_heads, axis=-1, keepdims=True)) + 1.0)
    value_heads = values.astype(jnp.float32).reshape(rows, -1, HEAD_DIM)
    write = unit * rate.reshape(rows, -1, HEAD_DIM)
    decay = jnp.exp(log_decay).reshape(rows, -1, HEAD_DIM)
    return (key_heads, value_heads, -unit, write, decay)

def run_chain(state, queries, inputs, reverse):
    key_heads, value_heads, erase, write, decay = inputs

    def advance(carry, item):
        query, key_row, value_row, erase_row, write_row, decay_row = item
        removed = jnp.einsum('hij,hj->hi', carry, erase_row, precision=highest)
        carry = carry * decay_row[:, None, :] + removed[:, :, None] * write_row[:, None, :] + value_row[:, :, None] * key_row[:, None, :]
        return (carry, jnp.einsum('hij,hj->hi', carry, query, precision=highest))
    return lax.scan(advance, state, (queries, key_heads, value_heads, erase, write, decay), reverse=reverse)

def reference(latent, context, condition, context_condition, shift_weight, scale_weight, gate_weight, norm_gain, decay_down, decay_up, rate_down, rate_up, head_bias, query_weight, key_weight, value_weight, branch_weight, group_gain, out_weight):
    conditions = jax.nn.silu(jnp.stack([condition, context_condition])).astype(jnp.bfloat16)
    shift = jnp.dot(conditions, shift_weight, preferred_element_type=jnp.float32)
    scale = jnp.dot(conditions, scale_weight, preferred_element_type=jnp.float32)
    gate = jnp.dot(conditions[:1], gate_weight, preferred_element_type=jnp.float32)[0]
    normed = modulated(latent, norm_gain, scale[0], shift[0])
    normed_context = modulated(context, norm_gain, scale[1], shift[1])
    queries = jnp.dot(normed, query_weight, preferred_element_type=jnp.float32).astype(jnp.bfloat16)
    branch = jnp.dot(normed, branch_weight, preferred_element_type=jnp.float32).astype(jnp.bfloat16)
    latent_in = chain_inputs(*features(normed, key_weight, value_weight, decay_down, decay_up, rate_down, rate_up), head_bias)
    context_in = chain_inputs(*features(normed_context, key_weight, value_weight, decay_down, decay_up, rate_down, rate_up), head_bias)
    query_heads = queries.astype(jnp.float32).reshape(TOKENS, -1, HEAD_DIM)
    zero_state = jnp.zeros((D // HEAD_DIM, HEAD_DIM, HEAD_DIM), jnp.float32)
    reads = jnp.zeros((TOKENS, D // HEAD_DIM, HEAD_DIM), jnp.float32)
    for reverse in (False, True):
        carried, _ = run_chain(zero_state, context_in[0], context_in, reverse)
        _, latent_read = run_chain(carried, query_heads, latent_in, reverse)
        reads = reads + latent_read
    center = lax.optimization_barrier(jnp.mean(reads, axis=-1, keepdims=True))
    variance = lax.optimization_barrier(jnp.mean(jnp.square(reads - center), axis=-1, keepdims=True))
    normal_heads = ((reads - center) * lax.rsqrt(variance + GROUP_EPS)).reshape(TOKENS, D)
    mixed = (normal_heads * group_gain * jax.nn.silu(branch.astype(jnp.float32))).astype(jnp.bfloat16)
    width = D // N_TP
    summed = jnp.zeros((TOKENS, D), jnp.float32)
    for group in range(N_TP):
        partial_sum = jnp.dot(mixed[:, group * width:(group + 1) * width], out_weight[group * width:(group + 1) * width], preferred_element_type=jnp.float32)
        summed = summed + lax.optimization_barrier(partial_sum.astype(jnp.bfloat16)).astype(jnp.float32)
    mixer = summed.astype(jnp.bfloat16).astype(jnp.float32)
    normed_out = mixer * lax.rsqrt(lax.optimization_barrier(jnp.mean(mixer * mixer, axis=-1, keepdims=True)) + NORM_EPS)
    return (latent.astype(jnp.float32) + gate * normed_out).astype(jnp.bfloat16)
```

```python
import functools
import math

import jax
import jax.numpy as jnp
from jax import lax
from jax.experimental import pallas as pl
from jax.experimental.pallas import tpu as pltpu
from jax.sharding import PartitionSpec as P

HEAD_DIM = 64
PAIR = 2 * HEAD_DIM
CHUNK = 64
GROUP = 2
NORM_EPS = 1e-06
GROUP_EPS = 0.00064
DECAY_TOP = math.exp(-0.5)
MOD_ROWS = 8
f32 = jnp.float32
bf16 = jnp.bfloat16


def dot(left, right, left_dim=1, right_dim=0):
    return lax.dot_general(
        left, right, (((left_dim,), (right_dim,)), ((), ())), preferred_element_type=f32
    )


def halves(value):
    high = value.astype(bf16)
    return high, (value - high.astype(f32)).astype(bf16)


def dot_fine(left, right):
    high, low = halves(left)
    return dot(high, right) + dot(low, right)


def iota(shape, dim):
    return lax.broadcasted_iota(jnp.int32, shape, dim)


def spread(packed):
    packed = packed.astype(f32)
    left = iota(packed.shape, 1) < HEAD_DIM
    zero = jnp.zeros_like(packed)
    return jnp.concatenate(
        [jnp.where(left, packed, zero), jnp.where(left, zero, packed)], axis=0
    ).astype(bf16)


def pick(full):
    left = iota((HEAD_DIM, PAIR), 1) < HEAD_DIM
    return jnp.where(left, full[:HEAD_DIM], full[HEAD_DIM:])


def same_head():
    return (iota((PAIR, PAIR), 0) < HEAD_DIM) == (iota((PAIR, PAIR), 1) < HEAD_DIM)


def chain_terms(keys, values, decay_pre, rate_pre, bias):
    log_decay = -DECAY_TOP * jax.nn.sigmoid(bias[0:1] + decay_pre.astype(f32))
    rate = jax.nn.sigmoid(bias[1:2] + rate_pre.astype(f32))
    keys = keys.astype(f32)
    ones = same_head().astype(f32).astype(bf16)
    unit = keys * lax.rsqrt(dot_fine(keys * keys, ones) + 1.0)
    return keys, values.astype(f32), -unit, unit * rate, log_decay


def cumulate(log_decay):
    rows = log_decay.shape[0]
    lower = (iota((rows, rows), 0) >= iota((rows, rows), 1)).astype(f32).astype(bf16)
    high, low = halves(log_decay)
    forward = dot(lower, high) + dot(lower, low)
    return forward, forward[rows - 1 : rows] - forward + log_decay


def chunk(terms, cumulative, flip, queries=None):
    keys, values, erase, write, log_decay = terms
    row = iota((CHUNK, PAIR), 0)
    col = iota((CHUNK, PAIR), 1) % HEAD_DIM
    before = (col > row) if flip else (col < row)
    until = (col >= row) if flip else (col <= row)
    final = cumulative[0:1] if flip else cumulative[CHUNK - 1 : CHUNK]
    erase_scaled = erase * jnp.exp(cumulative - log_decay)
    growth = jnp.exp(-cumulative)
    tail = jnp.exp(final - cumulative)
    left = erase_scaled.astype(bf16)
    if queries is not None:
        query_scaled = queries * jnp.exp(cumulative)
        left = jnp.concatenate([left, query_scaled.astype(bf16)], axis=0)
    right = jnp.concatenate([spread(write * growth), spread(keys * growth)], axis=0)
    products = dot(left, right, 1, 1)
    yield
    coupling = jnp.where(before, products[:CHUNK, :PAIR], 0.0)
    feeding = jnp.where(before, products[:CHUNK, PAIR:], 0.0)
    values_spread = spread(values)
    fed = dot(feeding.astype(bf16), values_spread)
    inverse = jnp.where(row == col, 1.0, jnp.where(row // 2 == col // 2, coupling, 0.0))
    yield
    size = 2
    while size < CHUNK:
        between = (row // (2 * size) == col // (2 * size)) & (row // size != col // size)
        step = dot(inverse.astype(bf16), spread(jnp.where(between, coupling, 0.0)))
        yield
        inverse = inverse + dot(step.astype(bf16), spread(inverse))
        yield
        size *= 2
    right = jnp.concatenate([spread(erase_scaled), spread(fed)], axis=1)
    solved = dot(inverse.astype(bf16), right)
    yield
    response, offset = solved[:, :PAIR], solved[:, PAIR:]
    write_tail = (write * tail).astype(bf16)
    key_tail = (keys * tail).astype(bf16)
    transfer = pick(dot(response.astype(bf16), write_tail, 0, 0))
    transfer = transfer + jnp.where(row == col, jnp.exp(final), 0.0)
    constant = pick(
        dot(
            jnp.concatenate([offset, values], axis=0).astype(bf16),
            jnp.concatenate([write_tail, key_tail], axis=0),
            0,
            0,
        )
    )
    if queries is None:
        return transfer, constant
    attend_write = jnp.where(until, products[CHUNK:, :PAIR], 0.0).astype(bf16)
    attend_key = jnp.where(until, products[CHUNK:, PAIR:], 0.0).astype(bf16)
    seen = dot(attend_write, jnp.concatenate([spread(response), spread(offset)], axis=1))
    yield
    factor = query_scaled + seen[:, :PAIR]
    read = seen[:, PAIR:] + dot(attend_key, values_spread)
    return transfer, constant, factor, read


def in_step(generators):
    results = [None] * len(generators)
    running = set(range(len(generators)))
    while running:
        for at in sorted(running):
            try:
                next(generators[at])
            except StopIteration as stop:
                results[at] = stop.value
                running.discard(at)
    return results


def modulation_kernel(condition, context_condition, shift, scale, gate, out):
    first = iota((16, condition.shape[1]), 0)
    stacked = jnp.where(first == 0, condition[...], 0.0)
    stacked = jnp.where(first == 1, context_condition[...], stacked)
    rows = jax.nn.silu(stacked).astype(bf16)
    parts = [dot(rows, weight[...]) for weight in (shift, scale, gate)]
    for at in range(out.shape[0]):
        for index, part in enumerate(parts):
            out[at, 2 * index : 2 * index + 2, :] = part[0:2]
        out[at, 6:8, :] = jnp.zeros((2, out.shape[2]), f32)


def local_kernel(pieces, *refs):
    latents = refs[:pieces]
    (context, mods, gain, decay_down, rate_down, decay_up, rate_up, bias) = refs[pieces : pieces + 8]
    weights = refs[pieces + 8 : pieces + 12]
    factors, reads, branch, maps, features, normed, low = refs[pieces + 12 :]
    own = latents[0].shape[0]
    rows = own * pieces
    context_rows = context.shape[0]
    rank = decay_down.shape[1]

    @pl.when(pl.program_id(0) == 0)
    def _():
        me = lax.axis_index("tp")
        blocks, _, width = mods.shape

        def norm(source, start, which):
            count = source.shape[0]
            total = jnp.zeros((count, 1), f32)
            for block in range(blocks):
                part = source[:, block * width : (block + 1) * width].astype(f32)
                total = total + jnp.sum(part * part, axis=-1, keepdims=True)
            inverse = lax.rsqrt(total / (blocks * width) + NORM_EPS)
            for block in range(blocks):
                columns = slice(block * width, (block + 1) * width)
                part = source[:, columns].astype(f32)
                factor = gain[:, columns] * (1.0 + mods[block, 2 + which : 3 + which, :])
                shifted = part * inverse * factor + mods[block, which : which + 1, :]
                normed[pl.ds(start, count), columns] = shifted.astype(bf16)

        for k in range(pieces):
            owner = lax.rem(me + (pieces - k), pieces)
            norm(latents[k], pl.multiple_of(owner * own, own), 0)
        norm(context, rows, 1)
        everything = normed[...]
        low[:, :rank] = jnp.tanh(dot(everything, decay_down[...])).astype(bf16)
        low[:, rank:] = dot(everything, rate_down[...]).astype(bf16)

    everything = normed[...]
    queries = dot(everything[:rows], weights[0][...]).astype(bf16)
    keys = dot(everything, weights[1][...]).astype(bf16)
    values = dot(everything, weights[2][...]).astype(bf16)
    branch[...] = dot(everything[:rows], weights[3][...]).astype(bf16)
    decay_pre = dot(low[:, :rank], decay_up[...]).astype(bf16)
    rate_pre = dot(low[:, rank:], rate_up[...]).astype(bf16)

    chunks = rows // CHUNK
    work = []
    for pair in range(GROUP):
        columns = slice(pair * PAIR, (pair + 1) * PAIR)
        for index, part in enumerate((keys, values, decay_pre, rate_pre)):
            features[pair, index] = part[rows:, columns]
        terms = chain_terms(
            keys[:rows, columns],
            values[:rows, columns],
            decay_pre[:rows, columns],
            rate_pre[:rows, columns],
            bias[:, columns],
        )
        pair_queries = queries[:, columns].astype(f32)
        for at in range(chunks):
            span = slice(at * CHUNK, (at + 1) * CHUNK)
            part = tuple(term[span] for term in terms)
            cumulative = cumulate(part[4])
            for flip in (0, 1):
                work.append(chunk(part, cumulative[flip], flip, pair_queries[span]))
    results = in_step(work)
    for pair in range(GROUP):
        total = [None] * chunks
        for flip in (0, 1):
            ahead = None
            for at in range(chunks)[:: -1 if flip else 1]:
                transfer, constant, factor, read = results[(pair * chunks + at) * 2 + flip]
                if ahead is None:
                    ahead = (transfer, constant)
                else:
                    through = dot(
                        factor.astype(bf16),
                        jnp.concatenate([spread(ahead[0]), spread(ahead[1])], axis=0),
                        1,
                        1,
                    )
                    factor = through[:, :PAIR]
                    read = read + through[:, PAIR:]
                    joined = dot_fine(jnp.concatenate(ahead, axis=0), spread(transfer))
                    ahead = (joined[:HEAD_DIM], joined[HEAD_DIM:] + constant)
                at_columns = (2 * pair + flip) * PAIR
                factors[at * CHUNK : (at + 1) * CHUNK, at_columns : at_columns + PAIR] = (
                    factor.astype(bf16)
                )
                total[at] = read if total[at] is None else total[at] + read
            maps[pair, flip, 0] = ahead[0].astype(bf16)
            maps[pair, flip, 1] = ahead[1].astype(bf16)
        for at in range(chunks):
            reads[at * CHUNK : (at + 1) * CHUNK, pair * PAIR : (pair + 1) * PAIR] = total[at]


def owner_kernel(features, bias, maps, starts):
    places = features.shape[0]
    parts = [
        jnp.concatenate([features[at, index] for at in range(places)], axis=0)
        for index in range(4)
    ]
    terms = chain_terms(parts[0], parts[1], parts[2], parts[3], bias[...])
    chunks = terms[0].shape[0] // CHUNK
    work = []
    for at in range(chunks):
        part = tuple(term[at * CHUNK : (at + 1) * CHUNK] for term in terms)
        cumulative = cumulate(part[4])
        for flip in (0, 1):
            work.append(chunk(part, cumulative[flip], flip))
    results = in_step(work)
    states = [None, None]
    for at in range(chunks):
        for flip in (0, 1):
            transfer, constant = results[(chunks - 1 - at if flip else at) * 2 + flip]
            if states[flip] is None:
                states[flip] = constant
            else:
                states[flip] = dot_fine(states[flip], spread(transfer)) + constant
    for at in range(places):
        for flip in (0, 1):
            place = places - 1 - at if flip else at
            starts[place, flip] = states[flip].astype(bf16)
            if at < places - 1:
                states[flip] = (
                    dot_fine(states[flip], spread(maps[place, flip, 0]))
                    + maps[place, flip, 1].astype(f32)
                )


def mix_kernel(reads, factors, branch, starts, gain, weight, out, held, mixed, sems):
    tiles = sems.shape[0]
    width = held.shape[1] // tiles
    copies = []
    for tile in range(tiles):
        columns = pl.ds(tile * width, width)
        copy = pltpu.make_async_copy(weight.at[:, columns], held.at[:, columns], sems.at[tile])
        copy.start()
        copies.append(copy)
    average = jnp.where(same_head(), 1.0 / HEAD_DIM, 0.0).astype(bf16)
    for pair in range(starts.shape[0]):
        columns = slice(pair * PAIR, (pair + 1) * PAIR)
        right = jnp.concatenate([spread(starts[pair, 0]), spread(starts[pair, 1])], axis=1)
        read = reads[:, columns] + dot(
            factors[:, 2 * pair * PAIR : 2 * (pair + 1) * PAIR], right, 1, 1
        )
        center = read - dot_fine(read, average)
        variance = dot_fine(center * center, average)
        normal = center * lax.rsqrt(variance + GROUP_EPS)
        gated = normal * gain[:, columns] * jax.nn.silu(branch[:, columns].astype(f32))
        mixed[:, columns] = gated.astype(bf16)
    rows = out.shape[1]
    for tile in range(tiles):
        copies[tile].wait()
        columns = slice(tile * width, (tile + 1) * width)
        part = dot(mixed[...], held[:, columns]).astype(bf16)
        for at in range(out.shape[0]):
            out[at, :, columns] = part[at * rows : (at + 1) * rows]


def finish_kernel(partials, latent, mods, out):
    blocks, _, width = mods.shape
    mixer = partials[0].astype(f32)
    for at in range(1, partials.shape[0]):
        mixer = mixer + partials[at].astype(f32)
    mixer = mixer.astype(bf16).astype(f32)
    inverse = lax.rsqrt(jnp.mean(mixer * mixer, axis=-1, keepdims=True) + NORM_EPS)
    normal = mixer * inverse
    for block in range(blocks):
        columns = slice(block * width, (block + 1) * width)
        gated = mods[block, 4:5, :] * normal[:, columns]
        out[:, columns] = (latent[:, columns].astype(f32) + gated).astype(bf16)


def cost(flops, moved):
    return pl.CostEstimate(flops=flops, bytes_accessed=moved, transcendentals=0)


def whole(array):
    return pl.BlockSpec(array.shape, lambda *_: (0,) * array.ndim)


def on_device(
    latent,
    context,
    condition,
    context_condition,
    shift_weight,
    scale_weight,
    gate_weight,
    norm_gain,
    decay_down,
    decay_up,
    rate_down,
    rate_up,
    head_bias,
    query_weight,
    key_weight,
    value_weight,
    branch_weight,
    group_gain,
    out_weight,
):
    places, columns_of = lax.axis_size("sp"), lax.axis_size("tp")
    model, local = query_weight.shape
    own = latent.shape[0]
    rows = own * columns_of
    context_rows = context.shape[0]
    rank = decay_down.shape[1]
    pairs = local // PAIR
    repeat = places // pairs
    assert places == repeat * pairs and rows % CHUNK == 0 and pairs % GROUP == 0

    latents = [latent]
    for k in range(1, columns_of):
        ring = [(i, (i + k) % columns_of) for i in range(columns_of)]
        latents.append(lax.ppermute(latent, "tp", ring))

    part = pl.pallas_call(
        modulation_kernel,
        out_shape=jax.ShapeDtypeStruct((places, MOD_ROWS, shift_weight.shape[1]), f32),
        cost_estimate=cost(2 * 16 * 3 * shift_weight.size, 6 * shift_weight.size),
        name="modulation",
    )(
        condition.reshape(1, -1),
        context_condition.reshape(1, -1),
        shift_weight,
        scale_weight,
        gate_weight,
    )
    summed = jnp.sum(lax.all_to_all(part, "sp", 0, 0), axis=0)
    mods = lax.all_gather(summed, "tp", axis=0)

    wide = GROUP * PAIR
    tile = lambda array: pl.BlockSpec((array.shape[0], wide), lambda g: (0, g))
    small = [context, mods, norm_gain.reshape(1, -1), decay_down, rate_down]
    tiled = [decay_up, rate_up, head_bias, query_weight, key_weight, value_weight, branch_weight]
    factors, reads, branch, maps, features = pl.pallas_call(
        functools.partial(local_kernel, columns_of),
        grid=(pairs // GROUP,),
        in_specs=[whole(a) for a in latents + small] + [tile(a) for a in tiled],
        out_specs=[
            pl.BlockSpec((rows, 2 * wide), lambda g: (0, g)),
            pl.BlockSpec((rows, wide), lambda g: (0, g)),
            pl.BlockSpec((rows, wide), lambda g: (0, g)),
            pl.BlockSpec((GROUP, 2, 2, HEAD_DIM, PAIR), lambda g: (g, 0, 0, 0, 0)),
            pl.BlockSpec((GROUP, 4, context_rows, PAIR), lambda g: (g, 0, 0, 0)),
        ],
        out_shape=[
            jax.ShapeDtypeStruct((rows, 2 * local), bf16),
            jax.ShapeDtypeStruct((rows, local), f32),
            jax.ShapeDtypeStruct((rows, local), bf16),
            jax.ShapeDtypeStruct((pairs, 2, 2, HEAD_DIM, PAIR), bf16),
            jax.ShapeDtypeStruct((pairs, 4, context_rows, PAIR), bf16),
        ],
        scratch_shapes=[
            pltpu.VMEM((rows + context_rows, model), bf16),
            pltpu.VMEM((rows + context_rows, 2 * rank), bf16),
        ],
        compiler_params=pltpu.CompilerParams(
            dimension_semantics=("arbitrary",), vmem_limit_bytes=56 * 2**20
        ),
        cost_estimate=cost(8 * rows * model * local, 8 * model * local),
        name="local",
    )(*latents, *small, *tiled)

    if repeat > 1:
        maps, features = jnp.repeat(maps, repeat, axis=0), jnp.repeat(features, repeat, axis=0)
    features = lax.all_to_all(features, "sp", 0, 0)
    maps = lax.all_to_all(maps, "sp", 0, 0)
    owned = lax.axis_index("sp") // repeat
    bias = lax.dynamic_slice(head_bias, (0, owned * PAIR), (2, PAIR))
    starts = pl.pallas_call(
        owner_kernel,
        out_shape=jax.ShapeDtypeStruct((places, 2, HEAD_DIM, PAIR), bf16),
        cost_estimate=cost(2**28, 2**20),
        name="owner",
    )(features, bias, maps)
    starts = lax.all_to_all(starts, "sp", 0, 0)[::repeat]

    tiles = 4
    partials = pl.pallas_call(
        mix_kernel,
        in_specs=[pl.BlockSpec(memory_space=pltpu.VMEM)] * 5 + [pl.BlockSpec(memory_space=pl.ANY)],
        out_specs=pl.BlockSpec(memory_space=pltpu.VMEM),
        out_shape=jax.ShapeDtypeStruct((columns_of, own, model), bf16),
        scratch_shapes=[
            pltpu.VMEM(out_weight.shape, bf16),
            pltpu.VMEM((rows, local), bf16),
            pltpu.SemaphoreType.DMA((tiles,)),
        ],
        cost_estimate=cost(2 * rows * local * model, 2 * local * model),
        name="mix",
    )(reads, factors, branch, starts, group_gain.reshape(1, -1), out_weight)
    partials = lax.all_to_all(partials, "tp", 0, 0)
    return pl.pallas_call(
        finish_kernel,
        out_shape=jax.ShapeDtypeStruct(latent.shape, bf16),
        cost_estimate=cost(latent.size * 16, latent.size * 12),
        name="finish",
    )(partials, latent, mods)


def solution(mesh):
    placed = (
        P(("sp", "tp"), None),
        P("sp", None),
        P("sp"),
        P("sp"),
        P("sp", "tp"),
        P("sp", "tp"),
        P("sp", "tp"),
        P(),
        P(),
        P(None, "tp"),
        P(),
        P(None, "tp"),
        P(None, "tp"),
        P(None, "tp"),
        P(None, "tp"),
        P(None, "tp"),
        P(None, "tp"),
        P("tp"),
        P("tp", None),
    )
    return jax.shard_map(
        on_device, mesh=mesh, in_specs=placed, out_specs=P(("sp", "tp"), None), check_vma=False
    )
```

```python
import functools
import math

import jax
import jax.numpy as jnp
from jax import lax
from jax.experimental import pallas as pl
from jax.experimental.pallas import tpu as pltpu
from jax.sharding import PartitionSpec as P

HEAD_DIM = 64
PAIR = 2 * HEAD_DIM
CHUNK = 64
GROUP = 2
NORM_EPS = 1e-06
GROUP_EPS = 0.00064
DECAY_TOP = math.exp(-0.5)
MOD_ROWS = 8
f32 = jnp.float32
bf16 = jnp.bfloat16


def dot(left, right, left_dim=1, right_dim=0):
    return lax.dot_general(
        left, right, (((left_dim,), (right_dim,)), ((), ())), preferred_element_type=f32
    )


def halves(value):
    high = value.astype(bf16)
    return high, (value - high.astype(f32)).astype(bf16)


def dot_fine(left, right):
    high, low = halves(left)
    return dot(high, right) + dot(low, right)


def iota(shape, dim):
    return lax.broadcasted_iota(jnp.int32, shape, dim)


def spread(packed):
    packed = packed.astype(f32)
    left = iota(packed.shape, 1) < HEAD_DIM
    zero = jnp.zeros_like(packed)
    return jnp.concatenate(
        [jnp.where(left, packed, zero), jnp.where(left, zero, packed)], axis=0
    ).astype(bf16)


def pick(full):
    left = iota((HEAD_DIM, PAIR), 1) < HEAD_DIM
    return jnp.where(left, full[:HEAD_DIM], full[HEAD_DIM:])


def same_head():
    return (iota((PAIR, PAIR), 0) < HEAD_DIM) == (iota((PAIR, PAIR), 1) < HEAD_DIM)


def chain_terms(keys, values, decay_pre, rate_pre, bias):
    log_decay = -DECAY_TOP * jax.nn.sigmoid(bias[0:1] + decay_pre.astype(f32))
    rate = jax.nn.sigmoid(bias[1:2] + rate_pre.astype(f32))
    keys = keys.astype(f32)
    ones = same_head().astype(f32).astype(bf16)
    unit = keys * lax.rsqrt(dot_fine(keys * keys, ones) + 1.0)
    return keys, values.astype(f32), -unit, unit * rate, log_decay


def cumulate(log_decay):
    rows = log_decay.shape[0]
    lower = (iota((rows, rows), 0) >= iota((rows, rows), 1)).astype(f32).astype(bf16)
    high, low = halves(log_decay)
    forward = dot(lower, high) + dot(lower, low)
    return forward, forward[rows - 1 : rows] - forward + log_decay


def chunk_masks(flip):
    row = iota((CHUNK, PAIR), 0)
    col = iota((CHUNK, PAIR), 1) % HEAD_DIM
    return row, col, (col > row) if flip else (col < row)


def chunk(terms, cumulative, flip):
    keys, values, erase, write, log_decay = terms
    row, col, before = chunk_masks(flip)
    final = cumulative[0:1] if flip else cumulative[CHUNK - 1 : CHUNK]
    erase_scaled = erase * jnp.exp(cumulative - log_decay)
    growth = jnp.exp(-cumulative)
    tail = jnp.exp(final - cumulative)
    write_scaled, key_scaled = write * growth, keys * growth
    right = jnp.concatenate([spread(write_scaled), spread(key_scaled)], axis=0)
    products = dot(erase_scaled.astype(bf16), right, 1, 1)
    yield
    coupling = jnp.where(before, products[:, :PAIR], 0.0)
    feeding = jnp.where(before, products[:, PAIR:], 0.0)
    fed = dot(feeding.astype(bf16), spread(values))
    inverse = jnp.where(row == col, 1.0, jnp.where(row // 2 == col // 2, coupling, 0.0))
    yield
    size = 2
    while size < CHUNK:
        between = (row // (2 * size) == col // (2 * size)) & (row // size != col // size)
        step = dot(inverse.astype(bf16), spread(jnp.where(between, coupling, 0.0)))
        yield
        inverse = inverse + dot(step.astype(bf16), spread(inverse))
        yield
        size *= 2
    right = jnp.concatenate([spread(erase_scaled), spread(fed)], axis=1)
    solved = dot(inverse.astype(bf16), right).astype(bf16)
    yield
    response, offset = solved[:, :PAIR], solved[:, PAIR:]
    write_tail = (write * tail).astype(bf16)
    key_tail = (keys * tail).astype(bf16)
    transfer = pick(dot(response, write_tail, 0, 0))
    transfer = transfer + jnp.where(row == col, jnp.exp(final), 0.0)
    constant = pick(
        dot(
            jnp.concatenate([offset, values.astype(bf16)], axis=0),
            jnp.concatenate([write_tail, key_tail], axis=0),
            0,
            0,
        )
    )
    kept = (write_scaled.astype(bf16), key_scaled.astype(bf16), response, offset)
    return transfer, constant, kept


def chunk_read(queries, values, kept, flip):
    row, col, before = chunk_masks(flip)
    until = before | (row == col)
    right = jnp.concatenate([spread(kept[0]), spread(kept[1])], axis=0)
    products = dot(queries.astype(bf16), right, 1, 1)
    yield
    attend_write = jnp.where(until, products[:, :PAIR], 0.0).astype(bf16)
    attend_key = jnp.where(until, products[:, PAIR:], 0.0).astype(bf16)
    seen = dot(attend_write, jnp.concatenate([spread(kept[2]), spread(kept[3])], axis=1))
    read = dot(attend_key, spread(values))
    yield
    return queries + seen[:, :PAIR], seen[:, PAIR:] + read


def in_step(generators):
    results = [None] * len(generators)
    running = set(range(len(generators)))
    while running:
        for at in sorted(running):
            try:
                next(generators[at])
            except StopIteration as stop:
                results[at] = stop.value
                running.discard(at)
    return results


def modulation_kernel(condition, context_condition, shift, scale, gate, out):
    first = iota((16, condition.shape[1]), 0)
    stacked = jnp.where(first == 0, condition[...], 0.0)
    stacked = jnp.where(first == 1, context_condition[...], stacked)
    rows = jax.nn.silu(stacked).astype(bf16)
    parts = [dot(rows, weight[...]) for weight in (shift, scale, gate)]
    for at in range(out.shape[0]):
        for index, part in enumerate(parts):
            out[at, 2 * index : 2 * index + 2, :] = part[0:2]
        out[at, 6:8, :] = jnp.zeros((2, out.shape[2]), f32)


def map_kernel(pieces, *refs):
    latents = refs[:pieces]
    context, mods, gain, decay_up, rate_up, bias = refs[pieces : pieces + 6]
    sources = refs[pieces + 6 : pieces + 10]
    package, value_out, kept, scales, firsts, normed = refs[pieces + 10 : pieces + 16]
    low_weight, weight, low, low_sems, sems = refs[pieces + 16 :]
    own = latents[0].shape[0]
    rows = own * pieces
    rank = decay_up.shape[0]
    steps = weight.shape[1]
    wide = weight.shape[3]
    step = pl.program_id(0)

    def low_copy(at):
        return pltpu.make_async_copy(sources[at], low_weight.at[at], low_sems.at[at])

    def weight_copy(at, tile):
        columns = pl.ds(tile * wide, wide)
        return pltpu.make_async_copy(
            sources[2 + at].at[:, columns], weight.at[at, tile], sems.at[at, tile]
        )

    @pl.when(step == 0)
    def _():
        for at in (0, 1):
            low_copy(at).start()
        for tile in range(steps):
            for at in (0, 1):
                weight_copy(at, tile).start()
        me = lax.axis_index("tp")
        blocks, _, width = mods.shape

        def norm(source, start, which):
            count = source.shape[0]
            total = jnp.zeros((count, 1), f32)
            for block in range(blocks):
                part = source[:, block * width : (block + 1) * width].astype(f32)
                total = total + jnp.sum(part * part, axis=-1, keepdims=True)
            inverse = lax.rsqrt(total / (blocks * width) + NORM_EPS)
            for block in range(blocks):
                columns = slice(block * width, (block + 1) * width)
                part = source[:, columns].astype(f32)
                factor = gain[:, columns] * (1.0 + mods[block, 2 + which : 3 + which, :])
                shifted = part * inverse * factor + mods[block, which : which + 1, :]
                normed[pl.ds(start, count), columns] = shifted.astype(bf16)

        for k in range(pieces):
            norm(latents[k], pl.multiple_of((me ^ k) * own, own), 0)
        norm(context, rows, 1)
        for at in (0, 1):
            low_copy(at).wait()
        everything = normed[...]
        low[:, :rank] = jnp.tanh(dot(everything, low_weight[0])).astype(bf16)
        low[:, rank:] = dot(everything, low_weight[1]).astype(bf16)

    for at in (0, 1):
        weight_copy(at, step).wait()
    everything = normed[...]
    keys = dot(everything, weight[0, step]).astype(bf16)
    values = dot(everything, weight[1, step]).astype(bf16)
    decay_pre = dot(low[:, :rank], decay_up[...]).astype(bf16)
    rate_pre = dot(low[:, rank:], rate_up[...]).astype(bf16)
    value_out[...] = values[:rows]

    chunks = rows // CHUNK
    feature_row = 4 * HEAD_DIM
    count = context.shape[0]
    work = []
    for pair in range(GROUP):
        columns = slice(pair * PAIR, (pair + 1) * PAIR)
        for index, part in enumerate((keys, values, decay_pre, rate_pre)):
            start = feature_row + index * count
            package[pair, start : start + count] = part[rows:, columns]
        terms = chain_terms(
            keys[:rows, columns],
            values[:rows, columns],
            decay_pre[:rows, columns],
            rate_pre[:rows, columns],
            bias[:, columns],
        )
        for at in range(chunks):
            part = tuple(term[at * CHUNK : (at + 1) * CHUNK] for term in terms)
            cumulative = cumulate(part[4])
            for flip in (0, 1):
                scales[pair, at, flip] = jnp.exp(cumulative[flip])
                work.append(chunk(part, cumulative[flip], flip))
    results = in_step(work)
    for pair in range(GROUP):
        for flip in (0, 1):
            ahead = None
            for at in range(chunks)[:: -1 if flip else 1]:
                transfer, constant, parts = results[(pair * chunks + at) * 2 + flip]
                for index, part in enumerate(parts):
                    kept[pair, at, flip, index] = part
                if ahead is None:
                    ahead = jnp.concatenate([transfer, constant], axis=0)
                else:
                    joined = dot_fine(ahead, spread(transfer))
                    ahead = jnp.concatenate(
                        [joined[:HEAD_DIM], joined[HEAD_DIM:] + constant], axis=0
                    )
                firsts[pair, at, flip] = ahead.astype(bf16)
            package[pair, flip * PAIR : (flip + 1) * PAIR] = ahead.astype(bf16)


def read_kernel(
    normed, query_weight, branch_weight, values, kept, scales, firsts, factors, reads, branch
):
    rows = values.shape[0]
    everything = normed[:rows]
    queries = dot(everything, query_weight[...]).astype(bf16).astype(f32)
    branch[...] = dot(everything, branch_weight[...]).astype(bf16)
    chunks = rows // CHUNK
    work = []
    for pair in range(GROUP):
        columns = slice(pair * PAIR, (pair + 1) * PAIR)
        for at in range(chunks):
            span = slice(at * CHUNK, (at + 1) * CHUNK)
            for flip in (0, 1):
                scaled = queries[span, columns] * scales[pair, at, flip]
                parts = [kept[pair, at, flip, index] for index in range(4)]
                work.append(chunk_read(scaled, values[span, columns], parts, flip))
    results = in_step(work)
    for pair in range(GROUP):
        for at in range(chunks):
            span = slice(at * CHUNK, (at + 1) * CHUNK)
            total = jnp.zeros((CHUNK, PAIR), f32)
            for flip in (0, 1):
                factor, read = results[(pair * chunks + at) * 2 + flip]
                earlier = at + 1 if flip else at - 1
                if 0 <= earlier < chunks:
                    ahead = firsts[pair, earlier, flip]
                    right = jnp.concatenate(
                        [spread(ahead[:HEAD_DIM]), spread(ahead[HEAD_DIM:])], axis=0
                    )
                    through = dot(factor.astype(bf16), right, 1, 1)
                    factor = through[:, :PAIR]
                    read = read + through[:, PAIR:]
                start = (2 * pair + flip) * PAIR
                factors[span, start : start + PAIR] = factor.astype(bf16)
                total = total + read
            reads[span, pair * PAIR : (pair + 1) * PAIR] = total


def owner_kernel(repeat, package, bias, after, starts):
    places = package.shape[0]
    feature_row = 4 * HEAD_DIM
    count = (package.shape[1] - feature_row) // 4
    parts = []
    for index in range(4):
        start = feature_row + index * count
        parts.append(
            jnp.concatenate([package[at, start : start + count] for at in range(places)], axis=0)
        )
    column = pl.multiple_of(lax.axis_index("sp") // repeat * PAIR, PAIR)
    own_bias = bias[:, pl.ds(column, PAIR)]
    terms = chain_terms(parts[0], parts[1], parts[2], parts[3], own_bias)
    chunks = terms[0].shape[0] // CHUNK
    work = []
    for at in range(chunks):
        part = tuple(term[at * CHUNK : (at + 1) * CHUNK] for term in terms)
        cumulative = cumulate(part[4])
        for flip in (0, 1):
            work.append(chunk(part, cumulative[flip], flip))
    results = in_step(work)
    states = [None, None]
    for at in range(chunks):
        for flip in (0, 1):
            transfer, constant, _ = results[(chunks - 1 - at if flip else at) * 2 + flip]
            if states[flip] is None:
                states[flip] = constant
            else:
                states[flip] = dot_fine(states[flip], spread(transfer)) + constant
    for at in range(places):
        for flip in (0, 1):
            place = places - 1 - at if flip else at
            starts[place, flip] = states[flip].astype(bf16)
            if at < places - 1:
                start = flip * PAIR
                transfer = package[place, start : start + HEAD_DIM]
                constant = package[place, start + HEAD_DIM : start + PAIR]
                states[flip] = dot_fine(states[flip], spread(transfer)) + constant.astype(f32)


def mix_kernel(reads, factors, branch, starts, gain, weight, keep, send, held, mixed, sems):
    tiles = sems.shape[0]
    width = held.shape[1] // tiles
    copies = []
    for tile in range(tiles):
        columns = pl.ds(tile * width, width)
        copy = pltpu.make_async_copy(weight.at[:, columns], held.at[:, columns], sems.at[tile])
        copy.start()
        copies.append(copy)
    blocks, rows, _ = keep.shape
    me = lax.axis_index("tp")
    average = jnp.where(same_head(), 1.0 / HEAD_DIM, 0.0).astype(bf16)
    for pair in range(starts.shape[0]):
        columns = slice(pair * PAIR, (pair + 1) * PAIR)
        right = jnp.concatenate([spread(starts[pair, 0]), spread(starts[pair, 1])], axis=1)
        read = reads[:, columns] + dot(
            factors[:, 2 * pair * PAIR : 2 * (pair + 1) * PAIR], right, 1, 1
        )
        center = read - dot_fine(read, average)
        variance = dot_fine(center * center, average)
        normal = center * lax.rsqrt(variance + GROUP_EPS)
        gated = normal * gain[:, columns] * jax.nn.silu(branch[:, columns].astype(f32))
        gated = gated.astype(bf16)
        for block in range(2 * blocks):
            start = (((block ^ me) & 1) * blocks + block // 2) * rows
            mixed[pl.ds(pl.multiple_of(start, rows), rows), columns] = gated[
                block * rows : (block + 1) * rows
            ]
    for tile in range(tiles):
        copies[tile].wait()
        columns = slice(tile * width, (tile + 1) * width)
        part = dot(mixed[...], held[:, columns]).astype(bf16)
        for block in range(blocks):
            keep[block, :, columns] = part[block * rows : (block + 1) * rows]
            send[block, :, columns] = part[(blocks + block) * rows : (blocks + block + 1) * rows]


def fold_kernel(bit, kept, came, keep, send):
    blocks = keep.shape[0]
    mine = (lax.axis_index("tp") >> bit) & 1
    for block in range(blocks):
        for out, at in ((keep, 2 * block + mine), (send, 2 * block + 1 - mine)):
            out[block] = (kept[at].astype(f32) + came[at].astype(f32)).astype(out.dtype)


def finish_kernel(kept, came, latent, mods, out):
    blocks, _, width = mods.shape
    mixer = (kept[0].astype(f32) + came[0].astype(f32)).astype(bf16).astype(f32)
    inverse = lax.rsqrt(jnp.mean(mixer * mixer, axis=-1, keepdims=True) + NORM_EPS)
    normal = mixer * inverse
    for block in range(blocks):
        columns = slice(block * width, (block + 1) * width)
        gated = mods[block, 4:5, :] * normal[:, columns]
        out[:, columns] = (latent[:, columns].astype(f32) + gated).astype(bf16)


def cost(flops, moved):
    return pl.CostEstimate(flops=flops, bytes_accessed=moved, transcendentals=0)


def in_hbm(*arrays):
    return [pltpu.with_memory_space_constraint(a, pltpu.HBM) for a in arrays]


def in_vmem(*arrays):
    return [pltpu.with_memory_space_constraint(a, pltpu.VMEM) for a in arrays]


def whole(array):
    return pl.BlockSpec(array.shape, lambda *_: (0,) * array.ndim)


def on_device(
    latent,
    context,
    condition,
    context_condition,
    shift_weight,
    scale_weight,
    gate_weight,
    norm_gain,
    decay_down,
    decay_up,
    rate_down,
    rate_up,
    head_bias,
    query_weight,
    key_weight,
    value_weight,
    branch_weight,
    group_gain,
    out_weight,
):
    places, columns_of = lax.axis_size("sp"), lax.axis_size("tp")
    model, local = query_weight.shape
    own = latent.shape[0]
    rows = own * columns_of
    context_rows = context.shape[0]
    rank = decay_down.shape[1]
    pairs = local // PAIR
    repeat = places // pairs
    assert places == repeat * pairs and rows % CHUNK == 0 and pairs % GROUP == 0

    bits = columns_of.bit_length() - 1
    assert columns_of == 1 << bits

    def swap(array, bit):
        return lax.ppermute(array, "tp", [(i, i ^ (1 << bit)) for i in range(columns_of)])

    latents = {0: latent}
    for bit in reversed(range(bits)):
        for k in list(latents):
            with jax.named_scope("gather"):
                latents[k | 1 << bit] = swap(latents[k], bit)
    latents = [latents[k] for k in range(columns_of)]

    part = pl.pallas_call(
        modulation_kernel,
        out_shape=jax.ShapeDtypeStruct((places, MOD_ROWS, shift_weight.shape[1]), f32),
        cost_estimate=cost(2 * 16 * 3 * shift_weight.size, 6 * shift_weight.size),
        compiler_params=pltpu.CompilerParams(vmem_limit_bytes=16 * 2**20),
        name="modulation",
    )(
        *in_hbm(
            condition.reshape(1, -1),
            context_condition.reshape(1, -1),
            shift_weight,
            scale_weight,
            gate_weight,
        )
    )
    summed = jnp.sum(lax.all_to_all(part, "sp", 0, 0), axis=0)
    mods = lax.all_gather(summed, "tp", axis=0)

    wide = GROUP * PAIR
    steps = pairs // GROUP
    chunks = rows // CHUNK
    package_rows = 4 * HEAD_DIM + 4 * context_rows
    tile = lambda array: pl.BlockSpec((array.shape[0], wide), lambda g: (0, g))
    lead = lambda *shape: pl.BlockSpec((GROUP,) + shape, lambda g: (g,) + (0,) * len(shape))
    anywhere = pl.BlockSpec(memory_space=pl.ANY)
    vmem_spec = pl.BlockSpec(memory_space=pltpu.VMEM)
    whole_in = latents + [context, mods, norm_gain.reshape(1, -1)]
    tiled = [decay_up, rate_up, head_bias]
    raw = [decay_down, rate_down, key_weight, value_weight]
    package, values, kept, scales, firsts, normed = pl.pallas_call(
        functools.partial(map_kernel, columns_of),
        grid=(steps,),
        in_specs=[whole(a) for a in whole_in] + [tile(a) for a in tiled] + [anywhere] * 4,
        out_specs=[
            lead(package_rows, PAIR),
            pl.BlockSpec((rows, wide), lambda g: (0, g)),
            lead(chunks, 2, 4, CHUNK, PAIR),
            lead(chunks, 2, CHUNK, PAIR),
            lead(chunks, 2, PAIR, PAIR),
            pl.BlockSpec((rows + context_rows, model), lambda g: (0, 0)),
        ],
        out_shape=[
            pltpu.HBM((pairs, package_rows, PAIR), bf16),
            pltpu.HBM((rows, local), bf16),
            pltpu.HBM((pairs, chunks, 2, 4, CHUNK, PAIR), bf16),
            pltpu.HBM((pairs, chunks, 2, CHUNK, PAIR), f32),
            pltpu.HBM((pairs, chunks, 2, PAIR, PAIR), bf16),
            pltpu.HBM((rows + context_rows, model), bf16),
        ],
        scratch_shapes=[
            pltpu.VMEM((2,) + decay_down.shape, bf16),
            pltpu.VMEM((2, steps, model, wide), bf16),
            pltpu.VMEM((rows + context_rows, 2 * rank), bf16),
            pltpu.SemaphoreType.DMA((2,)),
            pltpu.SemaphoreType.DMA((2, steps)),
        ],
        compiler_params=pltpu.CompilerParams(
            dimension_semantics=("arbitrary",), vmem_limit_bytes=36 * 2**20
        ),
        cost_estimate=cost(4 * rows * model * local, 4 * model * local),
        name="maps",
    )(
        *in_hbm(latents[0]),
        *in_vmem(*latents[1:]),
        *in_hbm(context),
        mods,
        *in_hbm(norm_gain.reshape(1, -1), *tiled, *raw),
    )

    if repeat > 1:
        package = jnp.repeat(package, repeat, axis=0)
    package = lax.all_to_all(package, "sp", 0, 0)

    factors, reads, branch = pl.pallas_call(
        read_kernel,
        grid=(steps,),
        in_specs=[
            whole(normed),
            tile(query_weight),
            tile(branch_weight),
            tile(values),
            lead(chunks, 2, 4, CHUNK, PAIR),
            lead(chunks, 2, CHUNK, PAIR),
            lead(chunks, 2, PAIR, PAIR),
        ],
        out_specs=[
            pl.BlockSpec((rows, 2 * wide), lambda g: (0, g)),
            pl.BlockSpec((rows, wide), lambda g: (0, g)),
            pl.BlockSpec((rows, wide), lambda g: (0, g)),
        ],
        out_shape=[
            pltpu.HBM((rows, 2 * local), bf16),
            pltpu.HBM((rows, local), f32),
            pltpu.HBM((rows, local), bf16),
        ],
        compiler_params=pltpu.CompilerParams(
            dimension_semantics=("arbitrary",), vmem_limit_bytes=24 * 2**20
        ),
        cost_estimate=cost(4 * rows * model * local, 4 * model * local),
        name="reads",
    )(*in_hbm(normed, query_weight, branch_weight, values, kept, scales, firsts))

    starts = pl.pallas_call(
        functools.partial(owner_kernel, repeat),
        in_specs=[vmem_spec, vmem_spec, anywhere],
        out_specs=vmem_spec,
        out_shape=jax.ShapeDtypeStruct((places, 2, HEAD_DIM, PAIR), bf16),
        cost_estimate=cost(2**28, 2**20),
        compiler_params=pltpu.CompilerParams(vmem_limit_bytes=16 * 2**20),
        name="owner",
    )(*in_vmem(package), *in_hbm(head_bias, branch))
    starts = lax.all_to_all(starts, "sp", 0, 0)[::repeat]

    tiles = 4
    half = pltpu.VMEM((columns_of // 2, own, model), bf16)
    keep, send = pl.pallas_call(
        mix_kernel,
        in_specs=[vmem_spec] * 5 + [anywhere],
        out_specs=[vmem_spec] * 2,
        out_shape=[half, half],
        scratch_shapes=[
            pltpu.VMEM(out_weight.shape, bf16),
            pltpu.VMEM((rows, local), bf16),
            pltpu.SemaphoreType.DMA((tiles,)),
        ],
        cost_estimate=cost(2 * rows * local * model, 2 * local * model),
        compiler_params=pltpu.CompilerParams(vmem_limit_bytes=24 * 2**20),
        name="mix",
    )(
        *in_hbm(reads, factors, branch),
        *in_vmem(starts),
        *in_hbm(group_gain.reshape(1, -1), out_weight),
    )
    for bit in range(bits):
        came = swap(send, bit)
        if bit < bits - 1:
            shape = (keep.shape[0] // 2,) + keep.shape[1:]
            keep, send = pl.pallas_call(
                functools.partial(fold_kernel, bit + 1),
                out_shape=[pltpu.VMEM(shape, f32), pltpu.VMEM(shape, bf16)],
                cost_estimate=cost(keep.size, 8 * keep.size),
                compiler_params=pltpu.CompilerParams(vmem_limit_bytes=8 * 2**20),
                name="fold",
            )(*in_vmem(keep, came))
    return pl.pallas_call(
        finish_kernel,
        out_shape=jax.ShapeDtypeStruct(latent.shape, bf16),
        cost_estimate=cost(latent.size * 16, latent.size * 12),
        compiler_params=pltpu.CompilerParams(vmem_limit_bytes=8 * 2**20),
        name="finish",
    )(*in_vmem(keep, came), *in_hbm(latent), mods)


def solution(mesh):
    placed = (
        P(("sp", "tp"), None),
        P("sp", None),
        P("sp"),
        P("sp"),
        P("sp", "tp"),
        P("sp", "tp"),
        P("sp", "tp"),
        P(),
        P(),
        P(None, "tp"),
        P(),
        P(None, "tp"),
        P(None, "tp"),
        P(None, "tp"),
        P(None, "tp"),
        P(None, "tp"),
        P(None, "tp"),
        P("tp"),
        P("tp", None),
    )
    return jax.shard_map(
        on_device, mesh=mesh, in_specs=placed, out_specs=P(("sp", "tp"), None), check_vma=False
    )
```

```python
import functools
import math

import jax
import jax.numpy as jnp
from jax import lax
from jax.experimental import pallas as pl
from jax.experimental.pallas import tpu as pltpu
from jax.sharding import PartitionSpec as P

HEAD_DIM = 64
PAIR = 2 * HEAD_DIM
CHUNK = 64
GROUP = 2
NORM_EPS = 1e-06
GROUP_EPS = 0.00064
DECAY_TOP = math.exp(-0.5)
MOD_ROWS = 5
f32 = jnp.float32
bf16 = jnp.bfloat16


def dot(left, right, left_dim=1, right_dim=0):
    return lax.dot_general(
        left, right, (((left_dim,), (right_dim,)), ((), ())), preferred_element_type=f32
    )


def halves(value):
    high = value.astype(bf16)
    return high, (value - high.astype(f32)).astype(bf16)


def dot_fine(left, right):
    high, low = halves(left)
    return dot(high, right) + dot(low, right)


def iota(shape, dim):
    return lax.broadcasted_iota(jnp.int32, shape, dim)


def spread(packed):
    packed = packed.astype(f32)
    left = iota(packed.shape, 1) < HEAD_DIM
    zero = jnp.zeros_like(packed)
    return jnp.concatenate(
        [jnp.where(left, packed, zero), jnp.where(left, zero, packed)], axis=0
    ).astype(bf16)


def pick(full):
    left = iota((HEAD_DIM, PAIR), 1) < HEAD_DIM
    return jnp.where(left, full[:HEAD_DIM], full[HEAD_DIM:])


def same_head():
    return (iota((PAIR, PAIR), 0) < HEAD_DIM) == (iota((PAIR, PAIR), 1) < HEAD_DIM)


def chain_terms(keys, values, decay_pre, rate_pre, bias):
    log_decay = -DECAY_TOP * jax.nn.sigmoid(bias[0:1] + decay_pre.astype(f32))
    rate = jax.nn.sigmoid(bias[1:2] + rate_pre.astype(f32))
    keys = keys.astype(f32)
    ones = same_head().astype(f32).astype(bf16)
    unit = keys * lax.rsqrt(dot_fine(keys * keys, ones) + 1.0)
    return keys, values.astype(f32), -unit, unit * rate, log_decay


def cumulate(log_decay):
    rows = log_decay.shape[0]
    lower = (iota((rows, rows), 0) >= iota((rows, rows), 1)).astype(f32).astype(bf16)
    high, low = halves(log_decay)
    forward = dot(lower, high) + dot(lower, low)
    return forward, forward[rows - 1 : rows] - forward + log_decay


def chunk_masks(flip):
    row = iota((CHUNK, PAIR), 0)
    col = iota((CHUNK, PAIR), 1) % HEAD_DIM
    return row, col, (col > row) if flip else (col < row)


def chunk(terms, cumulative, flip):
    keys, values, erase, write, log_decay = terms
    row, col, before = chunk_masks(flip)
    final = cumulative[0:1] if flip else cumulative[CHUNK - 1 : CHUNK]
    erase_scaled = erase * jnp.exp(cumulative - log_decay)
    growth = jnp.exp(-cumulative)
    tail = jnp.exp(final - cumulative)
    write_scaled, key_scaled = write * growth, keys * growth
    right = jnp.concatenate([spread(write_scaled), spread(key_scaled)], axis=0)
    products = dot(erase_scaled.astype(bf16), right, 1, 1)
    yield
    coupling = jnp.where(before, products[:, :PAIR], 0.0)
    feeding = jnp.where(before, products[:, PAIR:], 0.0)
    fed = dot(feeding.astype(bf16), spread(values))
    inverse = jnp.where(row == col, 1.0, jnp.where(row // 2 == col // 2, coupling, 0.0))
    yield
    size = 2
    while size < CHUNK:
        between = (row // (2 * size) == col // (2 * size)) & (row // size != col // size)
        step = dot(inverse.astype(bf16), spread(jnp.where(between, coupling, 0.0)))
        yield
        inverse = inverse + dot(step.astype(bf16), spread(inverse))
        yield
        size *= 2
    right = jnp.concatenate([spread(erase_scaled), spread(fed)], axis=1)
    solved = dot(inverse.astype(bf16), right).astype(bf16)
    yield
    response, offset = solved[:, :PAIR], solved[:, PAIR:]
    write_tail = (write * tail).astype(bf16)
    key_tail = (keys * tail).astype(bf16)
    transfer = pick(dot(response, write_tail, 0, 0))
    transfer = transfer + jnp.where(row == col, jnp.exp(final), 0.0)
    constant = pick(
        dot(
            jnp.concatenate([offset, values.astype(bf16)], axis=0),
            jnp.concatenate([write_tail, key_tail], axis=0),
            0,
            0,
        )
    )
    kept = (write_scaled.astype(bf16), key_scaled.astype(bf16), response, offset)
    return transfer, constant, kept


def chunk_read(queries, values, kept, flip):
    row, col, before = chunk_masks(flip)
    until = before | (row == col)
    right = jnp.concatenate([spread(kept[0]), spread(kept[1])], axis=0)
    products = dot(queries.astype(bf16), right, 1, 1)
    yield
    attend_write = jnp.where(until, products[:, :PAIR], 0.0).astype(bf16)
    attend_key = jnp.where(until, products[:, PAIR:], 0.0).astype(bf16)
    seen = dot(attend_write, jnp.concatenate([spread(kept[2]), spread(kept[3])], axis=1))
    read = dot(attend_key, spread(values))
    yield
    return queries + seen[:, :PAIR], seen[:, PAIR:] + read


def in_step(generators):
    results = [None] * len(generators)
    running = set(range(len(generators)))
    while running:
        for at in sorted(running):
            try:
                next(generators[at])
            except StopIteration as stop:
                results[at] = stop.value
                running.discard(at)
    return results


def modulation_kernel(condition, context_condition, shift, scale, gate, out):
    first = iota((16, condition.shape[1]), 0)
    stacked = jnp.where(first == 0, condition[...], 0.0)
    stacked = jnp.where(first == 1, context_condition[...], stacked)
    rows = jax.nn.silu(stacked).astype(bf16)
    parts = [dot(rows, weight[...]) for weight in (shift, scale, gate)]
    flat = [parts[0][0:1], parts[0][1:2], parts[1][0:1], parts[1][1:2], parts[2][0:1]]
    blocks = shift.shape[1] // PAIR
    for index, row in enumerate(flat):
        for block in range(blocks):
            at = index * blocks + block
            for place in range(out.shape[0]):
                out[place, at : at + 1, :] = row[:, block * PAIR : (block + 1) * PAIR]


def mod_row(mods, place, index):
    blocks = mods.shape[1] // MOD_ROWS
    start = index * blocks
    return jnp.concatenate(
        [mods[place, start + block : start + block + 1, :] for block in range(blocks)], axis=1
    )


def map_kernel(pieces, places, repeat, *refs):
    latents = refs[:pieces]
    context, mods, gain, decay_up, rate_up, bias = refs[pieces : pieces + 6]
    sources = refs[pieces + 6 : pieces + 10]
    packages = refs[pieces + 10 : pieces + 10 + places]
    value_out, kept, scales, firsts, normed, low, package = refs[pieces + 10 + places : -4]
    low_weight, weight, low_sems, sems = refs[-4:]
    steps = pl.num_programs(0)
    own = latents[0].shape[0]
    rows = own * pieces
    rank, wide = decay_up.shape
    step = pl.program_id(0)
    place = lax.axis_index("sp")

    def slot(pair, copy):
        owner = (step * GROUP + pair) * repeat + copy
        return lax.rem(owner - place + places, places)

    def low_copy(at):
        return pltpu.make_async_copy(sources[at], low_weight.at[at], low_sems.at[at])

    def weight_copies(tile):
        columns = pl.ds(pl.multiple_of(tile * wide, wide), wide)
        slot_at = lax.rem(tile, 2)
        parts = sems.shape[2]
        height = weight.shape[2] // parts
        copies = []
        for part in range(parts):
            span = pl.ds(part * height, height)
            for at in (0, 1):
                copies.append(
                    pltpu.make_async_copy(
                        sources[2 + at].at[span, columns],
                        weight.at[at, slot_at, span],
                        sems.at[at, slot_at, part],
                    )
                )
        return copies

    @pl.when(step == 0)
    def _():
        for at in (0, 1):
            low_copy(at).start()
        for copy in weight_copies(0):
            copy.start()
        me = lax.axis_index("tp")
        blocks = mods.shape[0]
        width = normed.shape[1] // blocks

        def norm(source, start, which):
            count = source.shape[0]
            total = jnp.zeros((count, 1), f32)
            for block in range(blocks):
                part = source[:, block * width : (block + 1) * width].astype(f32)
                total = total + jnp.sum(part * part, axis=-1, keepdims=True)
            inverse = lax.rsqrt(total / (blocks * width) + NORM_EPS)
            for block in range(blocks):
                columns = slice(block * width, (block + 1) * width)
                part = source[:, columns].astype(f32)
                factor = gain[:, columns] * (1.0 + mod_row(mods, block, 2 + which))
                shifted = part * inverse * factor + mod_row(mods, block, which)
                normed[pl.ds(start, count), columns] = shifted.astype(bf16)

        for k in range(pieces):
            norm(latents[k], pl.multiple_of((me ^ k) * own, own), 0)
        norm(context, rows, 1)
        for at in (0, 1):
            low_copy(at).wait()
        everything = normed[...]
        low[:, :rank] = jnp.tanh(dot(everything, low_weight[0])).astype(bf16)
        low[:, rank:] = dot(everything, low_weight[1]).astype(bf16)

    for copy in weight_copies(step):
        copy.wait()

    @pl.when(step + 1 < steps)
    def _():
        for copy in weight_copies(step + 1):
            copy.start()

    everything = normed[...]
    keys = dot(everything, weight[0, lax.rem(step, 2)]).astype(bf16)
    values = dot(everything, weight[1, lax.rem(step, 2)]).astype(bf16)
    decay_pre = dot(low[:, :rank], decay_up[...]).astype(bf16)
    rate_pre = dot(low[:, rank:], rate_up[...]).astype(bf16)
    value_out[...] = values[:rows]

    chunks = rows // CHUNK
    feature_row = 4 * HEAD_DIM
    count = context.shape[0]
    work = []
    for pair in range(GROUP):
        columns = slice(pair * PAIR, (pair + 1) * PAIR)
        for index, part in enumerate((keys, values, decay_pre, rate_pre)):
            start = feature_row + index * count
            for copy in range(repeat):
                package[slot(pair, copy), start : start + count] = part[rows:, columns]
        terms = chain_terms(
            keys[:rows, columns],
            values[:rows, columns],
            decay_pre[:rows, columns],
            rate_pre[:rows, columns],
            bias[:, columns],
        )
        for at in range(chunks):
            part = tuple(term[at * CHUNK : (at + 1) * CHUNK] for term in terms)
            cumulative = cumulate(part[4])
            for flip in (0, 1):
                scales[pair, at, flip] = jnp.exp(cumulative[flip])
                work.append(chunk(part, cumulative[flip], flip))
    results = in_step(work)
    for pair in range(GROUP):
        for flip in (0, 1):
            ahead = None
            for at in range(chunks)[:: -1 if flip else 1]:
                transfer, constant, parts = results[(pair * chunks + at) * 2 + flip]
                for index, part in enumerate(parts):
                    kept[pair, at, flip, index] = part
                if ahead is None:
                    ahead = jnp.concatenate([transfer, constant], axis=0)
                else:
                    joined = dot_fine(ahead, spread(transfer))
                    ahead = jnp.concatenate(
                        [joined[:HEAD_DIM], joined[HEAD_DIM:] + constant], axis=0
                    )
                firsts[pair, at, flip] = ahead.astype(bf16)
            for copy in range(repeat):
                span = slice(flip * PAIR, (flip + 1) * PAIR)
                package[slot(pair, copy), span] = ahead.astype(bf16)

    @pl.when(step == pl.num_programs(0) - 1)
    def _():
        for k in range(places):
            packages[k][...] = package[k]


def read_kernel(
    normed,
    query_weight,
    branch_weight,
    values,
    kept,
    scales,
    firsts,
    factors,
    reads,
    branch,
):
    rows = values.shape[0]
    step = pl.program_id(0)
    everything = normed[:rows]
    queries = dot(everything, query_weight[...]).astype(bf16).astype(f32)
    branch[...] = dot(everything, branch_weight[...]).astype(bf16)
    chunks = rows // CHUNK
    work = []
    for pair in range(GROUP):
        columns = slice(pair * PAIR, (pair + 1) * PAIR)
        for at in range(chunks):
            span = slice(at * CHUNK, (at + 1) * CHUNK)
            for flip in (0, 1):
                scaled = queries[span, columns] * scales[pair, at, flip]
                parts = [kept[pair, at, flip, index] for index in range(4)]
                work.append(chunk_read(scaled, values[span, columns], parts, flip))
    results = in_step(work)
    for pair in range(GROUP):
        for at in range(chunks):
            span = slice(at * CHUNK, (at + 1) * CHUNK)
            total = jnp.zeros((CHUNK, PAIR), f32)
            for flip in (0, 1):
                factor, read = results[(pair * chunks + at) * 2 + flip]
                earlier = at + 1 if flip else at - 1
                if 0 <= earlier < chunks:
                    ahead = firsts[pair, earlier, flip]
                    right = jnp.concatenate(
                        [spread(ahead[:HEAD_DIM]), spread(ahead[HEAD_DIM:])], axis=0
                    )
                    through = dot(factor.astype(bf16), right, 1, 1)
                    factor = through[:, :PAIR]
                    read = read + through[:, PAIR:]
                start = (2 * pair + flip) * PAIR
                factors[span, start : start + PAIR] = factor.astype(bf16)
                total = total + read
            reads[span, pair * PAIR : (pair + 1) * PAIR] = total


def owner_kernel(places, repeat, *refs):
    pieces, bias, outs = refs[:places], refs[places], refs[places + 2 : 2 * places + 2]
    package, starts = refs[2 * places + 2 :]
    me = lax.axis_index("sp")
    for k in range(places):
        package[lax.rem(me - k + places, places)] = pieces[k][...]
    feature_row = 4 * HEAD_DIM
    count = (package.shape[1] - feature_row) // 4
    parts = []
    for index in range(4):
        start = feature_row + index * count
        parts.append(
            jnp.concatenate([package[at, start : start + count] for at in range(places)], axis=0)
        )
    column = pl.multiple_of(me // repeat * PAIR, PAIR)
    own_bias = bias[:, pl.ds(column, PAIR)]
    terms = chain_terms(parts[0], parts[1], parts[2], parts[3], own_bias)
    chunks = terms[0].shape[0] // CHUNK
    work = []
    for at in range(chunks):
        part = tuple(term[at * CHUNK : (at + 1) * CHUNK] for term in terms)
        cumulative = cumulate(part[4])
        for flip in (0, 1):
            work.append(chunk(part, cumulative[flip], flip))
    results = in_step(work)
    states = [None, None]
    for at in range(chunks):
        for flip in (0, 1):
            transfer, constant, _ = results[(chunks - 1 - at if flip else at) * 2 + flip]
            if states[flip] is None:
                states[flip] = constant
            else:
                states[flip] = dot_fine(states[flip], spread(transfer)) + constant
    for at in range(places):
        for flip in (0, 1):
            place = places - 1 - at if flip else at
            starts[place, flip] = states[flip].astype(bf16)
            if at < places - 1:
                start = flip * PAIR
                transfer = package[place, start : start + HEAD_DIM]
                constant = package[place, start + HEAD_DIM : start + PAIR]
                states[flip] = dot_fine(states[flip], spread(transfer)) + constant.astype(f32)
    for k in range(places):
        outs[k][...] = starts[lax.rem(me + k, places)]


def mix_kernel(places, repeat, *refs):
    reads, factors, branch, gain, weight = refs[places : places + 5]
    keep, send, mixed, starts = refs[places + 5 :]
    at_place = lax.axis_index("sp")
    for k in range(places):
        starts[lax.rem(at_place - k + places, places)] = refs[k][...]
    tiles = 4
    width = weight.shape[1] // tiles
    blocks, rows, _ = keep.shape
    me = lax.axis_index("tp")
    average = jnp.where(same_head(), 1.0 / HEAD_DIM, 0.0).astype(bf16)
    for pair in range(places // repeat):
        own = pair * repeat
        columns = slice(pair * PAIR, (pair + 1) * PAIR)
        right = jnp.concatenate([spread(starts[own, 0]), spread(starts[own, 1])], axis=1)
        read = reads[:, columns] + dot(
            factors[:, 2 * pair * PAIR : 2 * (pair + 1) * PAIR], right, 1, 1
        )
        center = read - dot_fine(read, average)
        variance = dot_fine(center * center, average)
        normal = center * lax.rsqrt(variance + GROUP_EPS)
        gated = normal * gain[:, columns] * jax.nn.silu(branch[:, columns].astype(f32))
        gated = gated.astype(bf16)
        for block in range(2 * blocks):
            start = (((block ^ me) & 1) * blocks + block // 2) * rows
            mixed[pl.ds(pl.multiple_of(start, rows), rows), columns] = gated[
                block * rows : (block + 1) * rows
            ]
    for tile in range(tiles):
        columns = slice(tile * width, (tile + 1) * width)
        part = dot(mixed[...], weight[:, columns]).astype(bf16)
        for block in range(blocks):
            keep[block, :, columns] = part[block * rows : (block + 1) * rows]
            send[block, :, columns] = part[(blocks + block) * rows : (blocks + block + 1) * rows]


def fold_kernel(bit, kept, came, keep, send):
    blocks = keep.shape[0]
    mine = (lax.axis_index("tp") >> bit) & 1
    for block in range(blocks):
        for out, at in ((keep, 2 * block + mine), (send, 2 * block + 1 - mine)):
            out[block] = (kept[at].astype(f32) + came[at].astype(f32)).astype(out.dtype)


def finish_kernel(kept, came, latent, mods, out):
    blocks = mods.shape[0]
    width = out.shape[1] // blocks
    mixer = (kept[0].astype(f32) + came[0].astype(f32)).astype(bf16).astype(f32)
    inverse = lax.rsqrt(jnp.mean(mixer * mixer, axis=-1, keepdims=True) + NORM_EPS)
    normal = mixer * inverse
    for block in range(blocks):
        columns = slice(block * width, (block + 1) * width)
        gated = mod_row(mods, block, 4) * normal[:, columns]
        out[:, columns] = (latent[:, columns].astype(f32) + gated).astype(bf16)


def cost(flops, moved):
    return pl.CostEstimate(flops=flops, bytes_accessed=moved, transcendentals=0)


def in_hbm(*arrays):
    return [pltpu.with_memory_space_constraint(a, pltpu.HBM) for a in arrays]


def in_vmem(*arrays):
    return [pltpu.with_memory_space_constraint(a, pltpu.VMEM) for a in arrays]


def whole(array):
    return pl.BlockSpec(array.shape, lambda *_: (0,) * array.ndim)


def on_device(
    latent,
    context,
    condition,
    context_condition,
    shift_weight,
    scale_weight,
    gate_weight,
    norm_gain,
    decay_down,
    decay_up,
    rate_down,
    rate_up,
    head_bias,
    query_weight,
    key_weight,
    value_weight,
    branch_weight,
    group_gain,
    out_weight,
):
    places, columns_of = lax.axis_size("sp"), lax.axis_size("tp")
    model, local = query_weight.shape
    own = latent.shape[0]
    rows = own * columns_of
    context_rows = context.shape[0]
    rank = decay_down.shape[1]
    pairs = local // PAIR
    repeat = places // pairs
    assert places == repeat * pairs and rows % CHUNK == 0 and pairs % GROUP == 0

    bits = columns_of.bit_length() - 1
    assert columns_of == 1 << bits

    def ring(array, k):
        return lax.ppermute(array, "sp", [(i, (i + k) % places) for i in range(places)])

    def swap(array, bit):
        return lax.ppermute(array, "tp", [(i, i ^ (1 << bit)) for i in range(columns_of)])

    latents = {0: latent}
    for bit in reversed(range(bits)):
        for k in list(latents):
            with jax.named_scope("gather"):
                latents[k | 1 << bit] = swap(latents[k], bit)
    latents = [latents[k] for k in range(columns_of)]

    part = pl.pallas_call(
        modulation_kernel,
        out_shape=jax.ShapeDtypeStruct(
            (places, MOD_ROWS * shift_weight.shape[1] // PAIR, PAIR), f32
        ),
        cost_estimate=cost(2 * 16 * 3 * shift_weight.size, 6 * shift_weight.size),
        compiler_params=pltpu.CompilerParams(vmem_limit_bytes=16 * 2**20),
        name="modulation",
    )(
        *in_hbm(
            condition.reshape(1, -1),
            context_condition.reshape(1, -1),
            shift_weight,
            scale_weight,
            gate_weight,
        )
    )
    anywhere = pl.BlockSpec(memory_space=pl.ANY)
    vmem_spec = pl.BlockSpec(memory_space=pltpu.VMEM)
    summed = jnp.sum(lax.all_to_all(part, "sp", 0, 0), axis=0)
    mods = lax.all_gather(summed, "tp", axis=0)

    wide = GROUP * PAIR
    steps = pairs // GROUP
    chunks = rows // CHUNK
    package_rows = 4 * HEAD_DIM + 4 * context_rows
    tile = lambda array: pl.BlockSpec((array.shape[0], wide), lambda g: (0, g))
    lead = lambda *shape: pl.BlockSpec((GROUP,) + shape, lambda g: (g,) + (0,) * len(shape))
    whole_in = latents + [context, mods, norm_gain.reshape(1, -1)]
    tiled = [decay_up, rate_up, head_bias]
    raw = [decay_down, rate_down, key_weight, value_weight]
    *packages, values, kept, scales, firsts, normed = pl.pallas_call(
        functools.partial(map_kernel, columns_of, places, repeat),
        grid=(steps,),
        in_specs=[whole(a) for a in whole_in] + [tile(a) for a in tiled] + [anywhere] * 4,
        out_specs=[
            *[vmem_spec] * places,
            pl.BlockSpec((rows, wide), lambda g: (0, g)),
            lead(chunks, 2, 4, CHUNK, PAIR),
            lead(chunks, 2, CHUNK, PAIR),
            lead(chunks, 2, PAIR, PAIR),
            pl.BlockSpec((rows + context_rows, model), lambda g: (0, 0)),
        ],
        out_shape=[
            *[pltpu.VMEM((package_rows, PAIR), bf16)] * places,
            pltpu.VMEM((rows, local), bf16),
            pltpu.VMEM((pairs, chunks, 2, 4, CHUNK, PAIR), bf16),
            pltpu.VMEM((pairs, chunks, 2, CHUNK, PAIR), f32),
            pltpu.VMEM((pairs, chunks, 2, PAIR, PAIR), bf16),
            pltpu.VMEM((rows + context_rows, model), bf16),
        ],
        scratch_shapes=[
            pltpu.VMEM((rows + context_rows, 2 * rank), bf16),
            pltpu.VMEM((places, package_rows, PAIR), bf16),
            pltpu.VMEM((2,) + decay_down.shape, bf16),
            pltpu.VMEM((2, 2, model, wide), bf16),
            pltpu.SemaphoreType.DMA((2,)),
            pltpu.SemaphoreType.DMA((2, 2, 4)),
        ],
        compiler_params=pltpu.CompilerParams(
            dimension_semantics=("arbitrary",), vmem_limit_bytes=26 * 2**20
        ),
        cost_estimate=cost(4 * rows * model * local, 4 * model * local),
        name="maps",
    )(
        *in_hbm(latents[0]),
        *in_vmem(*latents[1:]),
        *in_hbm(context),
        mods,
        *in_hbm(norm_gain.reshape(1, -1), *tiled, *raw),
    )

    packages = packages[:1] + [ring(packages[k], k) for k in range(1, places)]

    factors, reads, branch = pl.pallas_call(
        read_kernel,
        grid=(steps,),
        in_specs=[
            whole(normed),
            tile(query_weight),
            tile(branch_weight),
            tile(values),
            lead(chunks, 2, 4, CHUNK, PAIR),
            lead(chunks, 2, CHUNK, PAIR),
            lead(chunks, 2, PAIR, PAIR),
        ],
        out_specs=[
            pl.BlockSpec((rows, 2 * wide), lambda g: (0, g)),
            pl.BlockSpec((rows, wide), lambda g: (0, g)),
            pl.BlockSpec((rows, wide), lambda g: (0, g)),
        ],
        out_shape=[
            pltpu.VMEM((rows, 2 * local), bf16),
            pltpu.VMEM((rows, local), f32),
            pltpu.VMEM((rows, local), bf16),
        ],
        compiler_params=pltpu.CompilerParams(
            dimension_semantics=("arbitrary",), vmem_limit_bytes=24 * 2**20
        ),
        cost_estimate=cost(4 * rows * model * local, 4 * model * local),
        name="reads",
    )(
        *in_vmem(normed),
        *in_hbm(query_weight, branch_weight),
        *in_vmem(values, kept, scales, firsts),
    )

    starts = pl.pallas_call(
        functools.partial(owner_kernel, places, repeat),
        in_specs=[vmem_spec] * (places + 1) + [anywhere],
        out_specs=[vmem_spec] * places,
        out_shape=[pltpu.VMEM((2, HEAD_DIM, PAIR), bf16)] * places,
        scratch_shapes=[
            pltpu.VMEM((places, package_rows, PAIR), bf16),
            pltpu.VMEM((places, 2, HEAD_DIM, PAIR), bf16),
        ],
        cost_estimate=cost(2**28, 2**20),
        compiler_params=pltpu.CompilerParams(vmem_limit_bytes=16 * 2**20),
        name="owner",
    )(*in_vmem(*packages), *in_hbm(head_bias), *in_vmem(branch))
    starts = [starts[0]] + [ring(starts[k], k) for k in range(1, places)]

    half = pltpu.VMEM((columns_of // 2, own, model), bf16)
    keep, send = pl.pallas_call(
        functools.partial(mix_kernel, places, repeat),
        in_specs=[vmem_spec] * (places + 5),
        out_specs=[vmem_spec] * 2,
        out_shape=[half, half],
        scratch_shapes=[
            pltpu.VMEM((rows, local), bf16),
            pltpu.VMEM((places, 2, HEAD_DIM, PAIR), bf16),
        ],
        cost_estimate=cost(2 * rows * local * model, 2 * local * model),
        compiler_params=pltpu.CompilerParams(vmem_limit_bytes=24 * 2**20),
        name="mix",
    )(
        *in_vmem(*starts),
        *in_vmem(reads, factors, branch),
        *in_hbm(group_gain.reshape(1, -1)),
        *in_vmem(out_weight),
    )
    for bit in range(bits):
        came = swap(send, bit)
        if bit < bits - 1:
            shape = (keep.shape[0] // 2,) + keep.shape[1:]
            keep, send = pl.pallas_call(
                functools.partial(fold_kernel, bit + 1),
                out_shape=[pltpu.VMEM(shape, f32), pltpu.VMEM(shape, bf16)],
                cost_estimate=cost(keep.size, 8 * keep.size),
                compiler_params=pltpu.CompilerParams(vmem_limit_bytes=8 * 2**20),
                name="fold",
            )(*in_vmem(keep, came))
    return pl.pallas_call(
        finish_kernel,
        out_shape=jax.ShapeDtypeStruct(latent.shape, bf16),
        cost_estimate=cost(latent.size * 16, latent.size * 12),
        compiler_params=pltpu.CompilerParams(vmem_limit_bytes=8 * 2**20),
        name="finish",
    )(*in_vmem(keep, came), *in_hbm(latent), mods)


def solution(mesh):
    placed = (
        P(("sp", "tp"), None),
        P("sp", None),
        P("sp"),
        P("sp"),
        P("sp", "tp"),
        P("sp", "tp"),
        P("sp", "tp"),
        P(),
        P(),
        P(None, "tp"),
        P(),
        P(None, "tp"),
        P(None, "tp"),
        P(None, "tp"),
        P(None, "tp"),
        P(None, "tp"),
        P(None, "tp"),
        P("tp"),
        P("tp", None),
    )
    return jax.shard_map(
        on_device, mesh=mesh, in_specs=placed, out_specs=P(("sp", "tp"), None), check_vma=False
    )
```

```python
import functools
import math

import jax
import jax.numpy as jnp
from jax import lax
from jax.experimental import pallas as pl
from jax.experimental.pallas import tpu as pltpu
from jax.sharding import PartitionSpec as P

HEAD_DIM = 64
PAIR = 2 * HEAD_DIM
CHUNK = 64
GROUP = 2
NORM_EPS = 1e-06
GROUP_EPS = 0.00064
DECAY_TOP = math.exp(-0.5)
MOD_ROWS = 5
f32 = jnp.float32
bf16 = jnp.bfloat16


def dot(left, right, left_dim=1, right_dim=0):
    return lax.dot_general(
        left, right, (((left_dim,), (right_dim,)), ((), ())), preferred_element_type=f32
    )


def halves(value):
    high = value.astype(bf16)
    return high, (value - high.astype(f32)).astype(bf16)


def dot_fine(left, right):
    high, low = halves(left)
    return dot(high, right) + dot(low, right)


def iota(shape, dim):
    return lax.broadcasted_iota(jnp.int32, shape, dim)


def spread(packed):
    packed = packed.astype(f32)
    left = iota(packed.shape, 1) < HEAD_DIM
    zero = jnp.zeros_like(packed)
    return jnp.concatenate(
        [jnp.where(left, packed, zero), jnp.where(left, zero, packed)], axis=0
    ).astype(bf16)


def pick(full):
    left = iota((HEAD_DIM, PAIR), 1) < HEAD_DIM
    return jnp.where(left, full[:HEAD_DIM], full[HEAD_DIM:])


def same_head():
    return (iota((PAIR, PAIR), 0) < HEAD_DIM) == (iota((PAIR, PAIR), 1) < HEAD_DIM)


def chain_terms(keys, values, decay_pre, rate_pre, bias):
    log_decay = -DECAY_TOP * jax.nn.sigmoid(bias[0:1] + decay_pre.astype(f32))
    rate = jax.nn.sigmoid(bias[1:2] + rate_pre.astype(f32))
    keys = keys.astype(f32)
    ones = same_head().astype(f32).astype(bf16)
    unit = keys * lax.rsqrt(dot_fine(keys * keys, ones) + 1.0)
    return keys, values.astype(f32), -unit, unit * rate, log_decay


def cumulate(log_decay):
    rows = log_decay.shape[0]
    lower = (iota((rows, rows), 0) >= iota((rows, rows), 1)).astype(f32).astype(bf16)
    high, low = halves(log_decay)
    forward = dot(lower, high) + dot(lower, low)
    return forward, forward[rows - 1 : rows] - forward + log_decay


def chunk_masks(flip):
    row = iota((CHUNK, PAIR), 0)
    col = iota((CHUNK, PAIR), 1) % HEAD_DIM
    return row, col, (col > row) if flip else (col < row)


def chunk(terms, cumulative, flip):
    keys, values, erase, write, log_decay = terms
    row, col, before = chunk_masks(flip)
    final = cumulative[0:1] if flip else cumulative[CHUNK - 1 : CHUNK]
    erase_scaled = erase * jnp.exp(cumulative - log_decay)
    growth = jnp.exp(-cumulative)
    tail = jnp.exp(final - cumulative)
    write_scaled, key_scaled = write * growth, keys * growth
    right = jnp.concatenate([spread(write_scaled), spread(key_scaled)], axis=0)
    products = dot(erase_scaled.astype(bf16), right, 1, 1)
    yield
    coupling = jnp.where(before, products[:, :PAIR], 0.0)
    feeding = jnp.where(before, products[:, PAIR:], 0.0)
    fed = dot(feeding.astype(bf16), spread(values))
    inverse = jnp.where(row == col, 1.0, jnp.where(row // 2 == col // 2, coupling, 0.0))
    yield
    size = 2
    while size < CHUNK:
        between = (row // (2 * size) == col // (2 * size)) & (row // size != col // size)
        step = dot(inverse.astype(bf16), spread(jnp.where(between, coupling, 0.0)))
        yield
        inverse = inverse + dot(step.astype(bf16), spread(inverse))
        yield
        size *= 2
    right = jnp.concatenate([spread(erase_scaled), spread(fed)], axis=1)
    solved = dot(inverse.astype(bf16), right).astype(bf16)
    yield
    response, offset = solved[:, :PAIR], solved[:, PAIR:]
    write_tail = (write * tail).astype(bf16)
    key_tail = (keys * tail).astype(bf16)
    transfer = pick(dot(response, write_tail, 0, 0))
    transfer = transfer + jnp.where(row == col, jnp.exp(final), 0.0)
    constant = pick(
        dot(
            jnp.concatenate([offset, values.astype(bf16)], axis=0),
            jnp.concatenate([write_tail, key_tail], axis=0),
            0,
            0,
        )
    )
    kept = (write_scaled.astype(bf16), key_scaled.astype(bf16), response, offset)
    return transfer, constant, kept


def chunk_read(queries, values, kept, flip):
    row, col, before = chunk_masks(flip)
    until = before | (row == col)
    right = jnp.concatenate([spread(kept[0]), spread(kept[1])], axis=0)
    products = dot(queries.astype(bf16), right, 1, 1)
    yield
    attend_write = jnp.where(until, products[:, :PAIR], 0.0).astype(bf16)
    attend_key = jnp.where(until, products[:, PAIR:], 0.0).astype(bf16)
    seen = dot(attend_write, jnp.concatenate([spread(kept[2]), spread(kept[3])], axis=1))
    read = dot(attend_key, spread(values))
    yield
    return queries + seen[:, :PAIR], seen[:, PAIR:] + read


def in_step(generators):
    results = [None] * len(generators)
    running = set(range(len(generators)))
    while running:
        for at in sorted(running):
            try:
                next(generators[at])
            except StopIteration as stop:
                results[at] = stop.value
                running.discard(at)
    return results


def modulation_kernel(condition, context_condition, shift, scale, gate, out):
    first = iota((16, condition.shape[1]), 0)
    stacked = jnp.where(first == 0, condition[...], 0.0)
    stacked = jnp.where(first == 1, context_condition[...], stacked)
    rows = jax.nn.silu(stacked).astype(bf16)
    parts = [dot(rows, weight[...]) for weight in (shift, scale, gate)]
    flat = [parts[0][0:1], parts[0][1:2], parts[1][0:1], parts[1][1:2], parts[2][0:1]]
    blocks = shift.shape[1] // PAIR
    for index, row in enumerate(flat):
        for block in range(blocks):
            at = index * blocks + block
            for place in range(out.shape[0]):
                out[place, at : at + 1, :] = row[:, block * PAIR : (block + 1) * PAIR]


def mod_row(mods, place, index):
    blocks = mods.shape[1] // MOD_ROWS
    start = index * blocks
    return jnp.concatenate(
        [mods[place, start + block : start + block + 1, :] for block in range(blocks)], axis=1
    )


def map_kernel(pieces, places, repeat, *refs):
    latents = refs[:pieces]
    context, mods, gain, decay_up, rate_up, bias = refs[pieces : pieces + 6]
    sources = refs[pieces + 6 : pieces + 10]
    packages = refs[pieces + 10 : pieces + 10 + places]
    value_out, kept, scales, firsts, normed, low, package = refs[pieces + 10 + places : -4]
    low_weight, weight, low_sems, sems = refs[-4:]
    steps = pl.num_programs(0)
    own = latents[0].shape[0]
    rows = own * pieces
    rank, wide = decay_up.shape
    step = pl.program_id(0)
    place = lax.axis_index("sp")

    def slot(pair, copy):
        owner = (step * GROUP + pair) * repeat + copy
        return lax.rem(owner - place + places, places)

    def low_copy(at):
        return pltpu.make_async_copy(sources[at], low_weight.at[at], low_sems.at[at])

    def weight_copies(tile):
        columns = pl.ds(pl.multiple_of(tile * wide, wide), wide)
        slot_at = lax.rem(tile, 2)
        parts = sems.shape[2]
        height = weight.shape[2] // parts
        copies = []
        for part in range(parts):
            span = pl.ds(part * height, height)
            for at in (0, 1):
                copies.append(
                    pltpu.make_async_copy(
                        sources[2 + at].at[span, columns],
                        weight.at[at, slot_at, span],
                        sems.at[at, slot_at, part],
                    )
                )
        return copies

    @pl.when(step == 0)
    def _():
        for at in (0, 1):
            low_copy(at).start()
        for copy in weight_copies(0):
            copy.start()
        me = lax.axis_index("tp")
        blocks = mods.shape[0]
        width = normed.shape[1] // blocks

        def norm(source, start, which):
            count = source.shape[0]
            total = jnp.zeros((count, 1), f32)
            for block in range(blocks):
                part = source[:, block * width : (block + 1) * width].astype(f32)
                total = total + jnp.sum(part * part, axis=-1, keepdims=True)
            inverse = lax.rsqrt(total / (blocks * width) + NORM_EPS)
            for block in range(blocks):
                columns = slice(block * width, (block + 1) * width)
                part = source[:, columns].astype(f32)
                factor = gain[:, columns] * (1.0 + mod_row(mods, block, 2 + which))
                shifted = part * inverse * factor + mod_row(mods, block, which)
                normed[pl.ds(start, count), columns] = shifted.astype(bf16)

        for k in range(pieces):
            norm(latents[k], pl.multiple_of((me ^ k) * own, own), 0)
        norm(context, rows, 1)
        for at in (0, 1):
            low_copy(at).wait()

        @pl.when(steps > 1)
        def _():
            for copy in weight_copies(1):
                copy.start()

        everything = normed[...]
        low[:, :rank] = jnp.tanh(dot(everything, low_weight[0])).astype(bf16)
        low[:, rank:] = dot(everything, low_weight[1]).astype(bf16)

    for copy in weight_copies(step):
        copy.wait()

    @pl.when((step > 0) & (step + 1 < steps))
    def _():
        for copy in weight_copies(step + 1):
            copy.start()

    everything = normed[...]
    keys = dot(everything, weight[0, lax.rem(step, 2)]).astype(bf16)
    values = dot(everything, weight[1, lax.rem(step, 2)]).astype(bf16)
    decay_pre = dot(low[:, :rank], decay_up[...]).astype(bf16)
    rate_pre = dot(low[:, rank:], rate_up[...]).astype(bf16)
    value_out[...] = values[:rows]

    chunks = rows // CHUNK
    feature_row = 4 * HEAD_DIM
    count = context.shape[0]
    work = []
    for pair in range(GROUP):
        columns = slice(pair * PAIR, (pair + 1) * PAIR)
        for index, part in enumerate((keys, values, decay_pre, rate_pre)):
            start = feature_row + index * count
            for copy in range(repeat):
                package[slot(pair, copy), start : start + count] = part[rows:, columns]
        terms = chain_terms(
            keys[:rows, columns],
            values[:rows, columns],
            decay_pre[:rows, columns],
            rate_pre[:rows, columns],
            bias[:, columns],
        )
        for at in range(chunks):
            part = tuple(term[at * CHUNK : (at + 1) * CHUNK] for term in terms)
            cumulative = cumulate(part[4])
            for flip in (0, 1):
                scales[pair, at, flip] = jnp.exp(cumulative[flip])
                work.append(chunk(part, cumulative[flip], flip))
    results = in_step(work)
    for pair in range(GROUP):
        for flip in (0, 1):
            ahead = None
            for at in range(chunks)[:: -1 if flip else 1]:
                transfer, constant, parts = results[(pair * chunks + at) * 2 + flip]
                for index, part in enumerate(parts):
                    kept[pair, at, flip, index] = part
                if ahead is None:
                    ahead = jnp.concatenate([transfer, constant], axis=0)
                else:
                    joined = dot_fine(ahead, spread(transfer))
                    ahead = jnp.concatenate(
                        [joined[:HEAD_DIM], joined[HEAD_DIM:] + constant], axis=0
                    )
                firsts[pair, at, flip] = ahead.astype(bf16)
            for copy in range(repeat):
                span = slice(flip * PAIR, (flip + 1) * PAIR)
                package[slot(pair, copy), span] = ahead.astype(bf16)

    @pl.when(step == pl.num_programs(0) - 1)
    def _():
        for k in range(places):
            packages[k][...] = package[k]


def read_kernel(
    normed,
    query_weight,
    branch_weight,
    values,
    kept,
    scales,
    firsts,
    factors,
    reads,
    branch,
):
    rows = values.shape[0]
    step = pl.program_id(0)
    everything = normed[:rows]
    queries = dot(everything, query_weight[...]).astype(bf16).astype(f32)
    branch[...] = dot(everything, branch_weight[...]).astype(bf16)
    chunks = rows // CHUNK
    work = []
    for pair in range(GROUP):
        columns = slice(pair * PAIR, (pair + 1) * PAIR)
        for at in range(chunks):
            span = slice(at * CHUNK, (at + 1) * CHUNK)
            for flip in (0, 1):
                scaled = queries[span, columns] * scales[pair, at, flip]
                parts = [kept[pair, at, flip, index] for index in range(4)]
                work.append(chunk_read(scaled, values[span, columns], parts, flip))
    results = in_step(work)
    for pair in range(GROUP):
        for at in range(chunks):
            span = slice(at * CHUNK, (at + 1) * CHUNK)
            total = jnp.zeros((CHUNK, PAIR), f32)
            for flip in (0, 1):
                factor, read = results[(pair * chunks + at) * 2 + flip]
                earlier = at + 1 if flip else at - 1
                if 0 <= earlier < chunks:
                    ahead = firsts[pair, earlier, flip]
                    right = jnp.concatenate(
                        [spread(ahead[:HEAD_DIM]), spread(ahead[HEAD_DIM:])], axis=0
                    )
                    through = dot(factor.astype(bf16), right, 1, 1)
                    factor = through[:, :PAIR]
                    read = read + through[:, PAIR:]
                start = (2 * pair + flip) * PAIR
                factors[span, start : start + PAIR] = factor.astype(bf16)
                total = total + read
            reads[span, pair * PAIR : (pair + 1) * PAIR] = total


def owner_kernel(places, repeat, *refs):
    pieces, bias, outs = refs[:places], refs[places], refs[places + 2 : 2 * places + 2]
    package, starts = refs[2 * places + 2 :]
    me = lax.axis_index("sp")
    for k in range(places):
        package[lax.rem(me - k + places, places)] = pieces[k][...]
    feature_row = 4 * HEAD_DIM
    count = (package.shape[1] - feature_row) // 4
    parts = []
    for index in range(4):
        start = feature_row + index * count
        parts.append(
            jnp.concatenate([package[at, start : start + count] for at in range(places)], axis=0)
        )
    column = pl.multiple_of(me // repeat * PAIR, PAIR)
    own_bias = bias[:, pl.ds(column, PAIR)]
    terms = chain_terms(parts[0], parts[1], parts[2], parts[3], own_bias)
    chunks = terms[0].shape[0] // CHUNK
    work = []
    for at in range(chunks):
        part = tuple(term[at * CHUNK : (at + 1) * CHUNK] for term in terms)
        cumulative = cumulate(part[4])
        for flip in (0, 1):
            work.append(chunk(part, cumulative[flip], flip))
    results = in_step(work)
    states = [None, None]
    for at in range(chunks):
        for flip in (0, 1):
            transfer, constant, _ = results[(chunks - 1 - at if flip else at) * 2 + flip]
            if states[flip] is None:
                states[flip] = constant
            else:
                states[flip] = dot_fine(states[flip], spread(transfer)) + constant
    for at in range(places):
        for flip in (0, 1):
            place = places - 1 - at if flip else at
            starts[place, flip] = states[flip].astype(bf16)
            if at < places - 1:
                start = flip * PAIR
                transfer = package[place, start : start + HEAD_DIM]
                constant = package[place, start + HEAD_DIM : start + PAIR]
                states[flip] = dot_fine(states[flip], spread(transfer)) + constant.astype(f32)
    for k in range(places):
        outs[k][...] = starts[lax.rem(me + k, places)]


def mix_kernel(places, repeat, *refs):
    reads, factors, branch, gain, weight = refs[places : places + 5]
    keep, send, mixed, starts = refs[places + 5 :]
    at_place = lax.axis_index("sp")
    for k in range(places):
        starts[lax.rem(at_place - k + places, places)] = refs[k][...]
    tiles = 4
    width = weight.shape[1] // tiles
    blocks, rows, _ = keep.shape
    me = lax.axis_index("tp")
    average = jnp.where(same_head(), 1.0 / HEAD_DIM, 0.0).astype(bf16)
    for pair in range(places // repeat):
        own = pair * repeat
        columns = slice(pair * PAIR, (pair + 1) * PAIR)
        right = jnp.concatenate([spread(starts[own, 0]), spread(starts[own, 1])], axis=1)
        read = reads[:, columns] + dot(
            factors[:, 2 * pair * PAIR : 2 * (pair + 1) * PAIR], right, 1, 1
        )
        center = read - dot_fine(read, average)
        variance = dot_fine(center * center, average)
        normal = center * lax.rsqrt(variance + GROUP_EPS)
        gated = normal * gain[:, columns] * jax.nn.silu(branch[:, columns].astype(f32))
        gated = gated.astype(bf16)
        for block in range(2 * blocks):
            start = (((block ^ me) & 1) * blocks + block // 2) * rows
            mixed[pl.ds(pl.multiple_of(start, rows), rows), columns] = gated[
                block * rows : (block + 1) * rows
            ]
    for tile in range(tiles):
        columns = slice(tile * width, (tile + 1) * width)
        part = dot(mixed[...], weight[:, columns]).astype(bf16)
        for block in range(blocks):
            keep[block, :, columns] = part[block * rows : (block + 1) * rows]
            send[block, :, columns] = part[(blocks + block) * rows : (blocks + block + 1) * rows]


def fold_kernel(bit, kept, came, keep, send):
    blocks = keep.shape[0]
    mine = (lax.axis_index("tp") >> bit) & 1
    for block in range(blocks):
        for out, at in ((keep, 2 * block + mine), (send, 2 * block + 1 - mine)):
            out[block] = (kept[at].astype(f32) + came[at].astype(f32)).astype(out.dtype)


def finish_kernel(kept, came, latent, mods, out):
    blocks = mods.shape[0]
    width = out.shape[1] // blocks
    mixer = (kept[0].astype(f32) + came[0].astype(f32)).astype(bf16).astype(f32)
    inverse = lax.rsqrt(jnp.mean(mixer * mixer, axis=-1, keepdims=True) + NORM_EPS)
    normal = mixer * inverse
    for block in range(blocks):
        columns = slice(block * width, (block + 1) * width)
        gated = mod_row(mods, block, 4) * normal[:, columns]
        out[:, columns] = (latent[:, columns].astype(f32) + gated).astype(bf16)


def cost(flops, moved):
    return pl.CostEstimate(flops=flops, bytes_accessed=moved, transcendentals=0)


def in_hbm(*arrays):
    return [pltpu.with_memory_space_constraint(a, pltpu.HBM) for a in arrays]


def in_vmem(*arrays):
    return [pltpu.with_memory_space_constraint(a, pltpu.VMEM) for a in arrays]


def whole(array):
    return pl.BlockSpec(array.shape, lambda *_: (0,) * array.ndim)


def on_device(
    latent,
    context,
    condition,
    context_condition,
    shift_weight,
    scale_weight,
    gate_weight,
    norm_gain,
    decay_down,
    decay_up,
    rate_down,
    rate_up,
    head_bias,
    query_weight,
    key_weight,
    value_weight,
    branch_weight,
    group_gain,
    out_weight,
):
    places, columns_of = lax.axis_size("sp"), lax.axis_size("tp")
    model, local = query_weight.shape
    own = latent.shape[0]
    rows = own * columns_of
    context_rows = context.shape[0]
    rank = decay_down.shape[1]
    pairs = local // PAIR
    repeat = places // pairs
    assert places == repeat * pairs and rows % CHUNK == 0 and pairs % GROUP == 0

    bits = columns_of.bit_length() - 1
    assert columns_of == 1 << bits

    def ring(array, k):
        return lax.ppermute(array, "sp", [(i, (i + k) % places) for i in range(places)])

    def swap(array, bit):
        return lax.ppermute(array, "tp", [(i, i ^ (1 << bit)) for i in range(columns_of)])

    latents = {0: latent}
    for bit in reversed(range(bits)):
        for k in list(latents):
            with jax.named_scope("gather"):
                latents[k | 1 << bit] = swap(latents[k], bit)
    latents = [latents[k] for k in range(columns_of)]

    part = pl.pallas_call(
        modulation_kernel,
        out_shape=jax.ShapeDtypeStruct(
            (places, MOD_ROWS * shift_weight.shape[1] // PAIR, PAIR), f32
        ),
        cost_estimate=cost(2 * 16 * 3 * shift_weight.size, 6 * shift_weight.size),
        compiler_params=pltpu.CompilerParams(vmem_limit_bytes=16 * 2**20),
        name="modulation",
    )(
        *in_hbm(
            condition.reshape(1, -1),
            context_condition.reshape(1, -1),
            shift_weight,
            scale_weight,
            gate_weight,
        )
    )
    anywhere = pl.BlockSpec(memory_space=pl.ANY)
    vmem_spec = pl.BlockSpec(memory_space=pltpu.VMEM)
    summed = jnp.sum(lax.all_to_all(part, "sp", 0, 0), axis=0)
    mods = lax.all_gather(summed, "tp", axis=0)

    wide = GROUP * PAIR
    steps = pairs // GROUP
    chunks = rows // CHUNK
    package_rows = 4 * HEAD_DIM + 4 * context_rows
    tile = lambda array: pl.BlockSpec((array.shape[0], wide), lambda g: (0, g))
    lead = lambda *shape: pl.BlockSpec((GROUP,) + shape, lambda g: (g,) + (0,) * len(shape))
    whole_in = latents + [context, mods, norm_gain.reshape(1, -1)]
    tiled = [decay_up, rate_up, head_bias]
    raw = [decay_down, rate_down, key_weight, value_weight]
    *packages, values, kept, scales, firsts, normed = pl.pallas_call(
        functools.partial(map_kernel, columns_of, places, repeat),
        grid=(steps,),
        in_specs=[whole(a) for a in whole_in] + [tile(a) for a in tiled] + [anywhere] * 4,
        out_specs=[
            *[vmem_spec] * places,
            pl.BlockSpec((rows, wide), lambda g: (0, g)),
            lead(chunks, 2, 4, CHUNK, PAIR),
            lead(chunks, 2, CHUNK, PAIR),
            lead(chunks, 2, PAIR, PAIR),
            pl.BlockSpec((rows + context_rows, model), lambda g: (0, 0)),
        ],
        out_shape=[
            *[pltpu.VMEM((package_rows, PAIR), bf16)] * places,
            pltpu.VMEM((rows, local), bf16),
            pltpu.VMEM((pairs, chunks, 2, 4, CHUNK, PAIR), bf16),
            pltpu.VMEM((pairs, chunks, 2, CHUNK, PAIR), f32),
            pltpu.VMEM((pairs, chunks, 2, PAIR, PAIR), bf16),
            pltpu.VMEM((rows + context_rows, model), bf16),
        ],
        scratch_shapes=[
            pltpu.VMEM((rows + context_rows, 2 * rank), bf16),
            pltpu.VMEM((places, package_rows, PAIR), bf16),
            pltpu.VMEM((2,) + decay_down.shape, bf16),
            pltpu.VMEM((2, 2, model, wide), bf16),
            pltpu.SemaphoreType.DMA((2,)),
            pltpu.SemaphoreType.DMA((2, 2, 4)),
        ],
        compiler_params=pltpu.CompilerParams(
            dimension_semantics=("arbitrary",), vmem_limit_bytes=26 * 2**20
        ),
        cost_estimate=cost(4 * rows * model * local, 4 * model * local),
        name="maps",
    )(
        *in_hbm(latents[0]),
        *in_vmem(*latents[1:]),
        *in_hbm(context),
        mods,
        *in_hbm(norm_gain.reshape(1, -1), *tiled, *raw),
    )

    sent = {k: ring(packages[k], k) for k in sorted(range(1, places), key=lambda k: abs(2 * k - places))}
    packages = [packages[0]] + [sent[k] for k in range(1, places)]

    factors, reads, branch = pl.pallas_call(
        read_kernel,
        grid=(steps,),
        in_specs=[
            whole(normed),
            tile(query_weight),
            tile(branch_weight),
            tile(values),
            lead(chunks, 2, 4, CHUNK, PAIR),
            lead(chunks, 2, CHUNK, PAIR),
            lead(chunks, 2, PAIR, PAIR),
        ],
        out_specs=[
            pl.BlockSpec((rows, 2 * wide), lambda g: (0, g)),
            pl.BlockSpec((rows, wide), lambda g: (0, g)),
            pl.BlockSpec((rows, wide), lambda g: (0, g)),
        ],
        out_shape=[
            pltpu.VMEM((rows, 2 * local), bf16),
            pltpu.VMEM((rows, local), f32),
            pltpu.VMEM((rows, local), bf16),
        ],
        compiler_params=pltpu.CompilerParams(
            dimension_semantics=("arbitrary",), vmem_limit_bytes=24 * 2**20
        ),
        cost_estimate=cost(4 * rows * model * local, 4 * model * local),
        name="reads",
    )(
        *in_vmem(normed),
        *in_hbm(query_weight, branch_weight),
        *in_vmem(values, kept, scales, firsts),
    )

    starts = pl.pallas_call(
        functools.partial(owner_kernel, places, repeat),
        in_specs=[vmem_spec] * (places + 1) + [anywhere],
        out_specs=[vmem_spec] * places,
        out_shape=[pltpu.VMEM((2, HEAD_DIM, PAIR), bf16)] * places,
        scratch_shapes=[
            pltpu.VMEM((places, package_rows, PAIR), bf16),
            pltpu.VMEM((places, 2, HEAD_DIM, PAIR), bf16),
        ],
        cost_estimate=cost(2**28, 2**20),
        compiler_params=pltpu.CompilerParams(vmem_limit_bytes=16 * 2**20),
        name="owner",
    )(*in_vmem(*packages), *in_hbm(head_bias), *in_vmem(branch))
    sent = {k: ring(starts[k], k) for k in sorted(range(1, places), key=lambda k: abs(2 * k - places))}
    starts = [starts[0]] + [sent[k] for k in range(1, places)]

    half = pltpu.VMEM((columns_of // 2, own, model), bf16)
    keep, send = pl.pallas_call(
        functools.partial(mix_kernel, places, repeat),
        in_specs=[vmem_spec] * (places + 5),
        out_specs=[vmem_spec] * 2,
        out_shape=[half, half],
        scratch_shapes=[
            pltpu.VMEM((rows, local), bf16),
            pltpu.VMEM((places, 2, HEAD_DIM, PAIR), bf16),
        ],
        cost_estimate=cost(2 * rows * local * model, 2 * local * model),
        compiler_params=pltpu.CompilerParams(vmem_limit_bytes=24 * 2**20),
        name="mix",
    )(
        *in_vmem(*starts),
        *in_vmem(reads, factors, branch),
        *in_hbm(group_gain.reshape(1, -1)),
        *in_vmem(out_weight),
    )
    for bit in range(bits):
        came = swap(send, bit)
        if bit < bits - 1:
            shape = (keep.shape[0] // 2,) + keep.shape[1:]
            keep, send = pl.pallas_call(
                functools.partial(fold_kernel, bit + 1),
                out_shape=[pltpu.VMEM(shape, f32), pltpu.VMEM(shape, bf16)],
                cost_estimate=cost(keep.size, 8 * keep.size),
                compiler_params=pltpu.CompilerParams(vmem_limit_bytes=8 * 2**20),
                name="fold",
            )(*in_vmem(keep, came))
    return pl.pallas_call(
        finish_kernel,
        out_shape=jax.ShapeDtypeStruct(latent.shape, bf16),
        cost_estimate=cost(latent.size * 16, latent.size * 12),
        compiler_params=pltpu.CompilerParams(vmem_limit_bytes=8 * 2**20),
        name="finish",
    )(*in_vmem(keep, came, latent), mods)


def solution(mesh):
    placed = (
        P(("sp", "tp"), None),
        P("sp", None),
        P("sp"),
        P("sp"),
        P("sp", "tp"),
        P("sp", "tp"),
        P("sp", "tp"),
        P(),
        P(),
        P(None, "tp"),
        P(),
        P(None, "tp"),
        P(None, "tp"),
        P(None, "tp"),
        P(None, "tp"),
        P(None, "tp"),
        P(None, "tp"),
        P("tp"),
        P("tp", None),
    )
    return jax.shard_map(
        on_device, mesh=mesh, in_specs=placed, out_specs=P(("sp", "tp"), None), check_vma=False
    )
```
